256 devices in a mesh: sp: 64 (over z, x, core), tp: 4 (over y).
Axes of the slice: x: 4, y: 4, z: 8, core: 2. Of those that a mesh axis runs over, the one named last changes fastest.
Arguments:
- residual: bfloat16 [8192, 2048], P(('sp', 'tp')), may hold values from -20 to 20
- query_small: bfloat16 [8192, 384], P('sp', 'tp'), may hold values from -12 to 12
- query_large: bfloat16 [8192, 640], P('sp', 'tp'), may hold values from -12 to 12
- latent: bfloat16 [8192, 512], P('sp'), may hold values from -30 to 30
- rotary_key: bfloat16 [8192, 32], P('sp'), may hold values from -16 to 16
- latent_gain: float32 [512], replicated, may hold values from 0.1 to 1.9
- small_keys: bfloat16 [512, 256], P(None, 'tp'), may hold values from -0.25 to 0.25
- small_values: bfloat16 [512, 256], P(None, 'tp'), may hold values from -0.25 to 0.25
- large_keys: bfloat16 [512, 512], P(None, 'tp'), may hold values from -0.25 to 0.25
- large_values: bfloat16 [512, 512], P(None, 'tp'), may hold values from -0.25 to 0.25
- small_output: bfloat16 [256, 2048], P('tp'), may hold values from -0.21875 to 0.21875
- large_output: bfloat16 [512, 2048], P('tp'), may hold values from -0.21875 to 0.21875
- ffn_gain: float32 [2048], replicated, may hold values from 0.1 to 1.9
- gate_weights: bfloat16 [64, 2048, 2048], P('sp', None, 'tp'), may hold values from -2 to 2
- up_weights: bfloat16 [64, 2048, 2048], P('sp', None, 'tp'), may hold values from -2 to 2
- down_weights: bfloat16 [64, 2048, 2048], P('sp', 'tp'), may hold values from -0.046875 to 0.046875
- routing: int32 [8192, 2], P(('sp', 'tp')), may hold values from 0 to 63, all different within a row; in each aligned block of 32 rows (0 to 31, 32 to 63, ...) at most 2 rows name the same one
- route_weight: float32 [8192, 2], P(('sp', 'tp')), may hold values from 0.2 to 1
Outputs:
- output: bfloat16 [8192, 2048], P(('sp', 'tp'))
The draws below stay inside these ranges and needn't reach their ends.
Inputs may be any that keep to these rules, and one draw needn't show every extreme that they name: `routing`: each row names 2 different experts. Within the rows of one device (aligned blocks of 32 rows) no expert is named by more than 2 rows, and in every draw some block has an expert named by exactly 2 rows.
All inputs are finite; a program needn't handle non-finite values.
Results may differ from the reference program's by a relative error of at most 0.018.
Values may be sent and summed in bfloat16 or wider, within the bound.
No kernel may reach another device: no remote copies, remote signals or barrier semaphores. Data moves between devices by JAX's collectives and lax.ppermute only.
A program may use at most 128 MiB of HBM per device.

```python
import math
import jax
import jax.numpy as jnp
import numpy as np
from jax import lax

D = 2048
LATENT = 512
HEADS_S = 4
HEADS_L = 4
NOPE_S = 64
V_S = 64
NOPE_L = 128
V_L = 128
ROPE = 32
FF = 2048
TOPK = 2
TOK_DEV = 32
SEQ_LEN = 8192
EXPERTS = 64
CAP = 2
N_SP = 64
N_TP = 4


def scaled_rows(key, row_count, col_count, row_low, row_high, col_low, col_high):
    sub_keys = jax.random.split(jax.random.fold_in(key, 11), 3)
    base = jnp.clip(jax.random.normal(sub_keys[0], (row_count, col_count), jnp.float32), -5.0, 5.0)
    row_scale = jnp.exp(jax.random.uniform(sub_keys[1], (row_count, 1), jnp.float32, math.log(row_low), math.log(row_high)))
    col_scale = jnp.exp(jax.random.uniform(sub_keys[2], (1, col_count), jnp.float32, math.log(col_low), math.log(col_high)))
    return base * row_scale * col_scale


def draw_queries(key, head_count, nope, salt):
    width = nope + ROPE
    own_key = jax.random.fold_in(key, salt)
    whole = jnp.clip(2.5 * jax.random.normal(own_key, (SEQ_LEN, head_count, width), jnp.float32), -12.0, 12.0)
    return whole.reshape(SEQ_LEN, head_count * width)


def draw_query_small(key, part):
    return draw_queries(key, HEADS_S, NOPE_S, 21).astype(jnp.bfloat16)


def draw_query_large(key, part):
    return draw_queries(key, HEADS_L, NOPE_L, 22).astype(jnp.bfloat16)


def draw_rotary_key(key, part):
    own_key = jax.random.fold_in(key, 31)
    base = jnp.clip(jax.random.normal(own_key, (SEQ_LEN, ROPE), jnp.float32), -6.0, 6.0)
    return base.astype(jnp.bfloat16)


def draw_residual(key, part):
    return scaled_rows(jax.random.fold_in(key, 41), SEQ_LEN, D, 0.5, 2.0, 0.5, 2.0).astype(jnp.bfloat16)


def draw_latent(key, part):
    return scaled_rows(jax.random.fold_in(key, 42), SEQ_LEN, LATENT, 0.3, 3.0, 0.5, 2.0).astype(jnp.bfloat16)


def expert_matrix(key, salt):
    own_key = jax.random.fold_in(key, salt)
    return jnp.clip(jax.random.normal(own_key, (EXPERTS, D, FF), jnp.float32), -6.0, 6.0) * (2.5 / math.sqrt(D))


def draw_gate_weights(key, part):
    return expert_matrix(key, 51).astype(jnp.bfloat16)


def draw_up_weights(key, part):
    return expert_matrix(key, 52).astype(jnp.bfloat16)


def block_levels(stream_key, dims, cuts, low, high):
    level = 1.0
    for position, parts in cuts:
        draws = jax.random.uniform(jax.random.fold_in(jax.random.fold_in(stream_key, 6), position), (parts,), jnp.float32, low / len(cuts), high / len(cuts))
        level = level * jnp.repeat(jnp.exp(draws), dims[position] // parts).reshape((-1,) + (1,) * (len(dims) - 1 - position))
    return level


def shared_out(key, own, number, rows, count, top, reach, skew):
    order = jax.random.permutation(key, count)
    crowded, ordinary = load_shares(count, rows * top, reach, skew, True), load_shares(count, rows * top, reach, skew, False)
    places = jnp.arange(count)

    def named(lengths, offset_by):
        used = int((lengths > 0).sum())
        fixed = max(1, used // 4)
        moved = fixed + (places - fixed + offset_by * (used - fixed)) % max(1, count - fixed)
        return jnp.zeros((count,), jnp.int32).at[order[jnp.where(places < fixed, places, moved)]].set(jnp.asarray(lengths, jnp.int32))

    lengths = jnp.where(number % 4 == 0, named(crowded, number // 4), named(ordinary, number - number // 4 - 1))
    mixed = jax.random.permutation(jax.random.fold_in(own, 3), count)
    source_of, receiver = mixed[0:count // 2 * 2:2], mixed[1:count // 2 * 2:2]
    slack = jnp.minimum(lengths[source_of] - 1, reach - lengths[receiver]) // 2
    slack = jnp.where((source_of == order[0]) | (receiver == order[0]) | (lengths[receiver] == 0), 0, jnp.maximum(slack, 0))
    moved = jax.random.randint(jax.random.fold_in(own, 4), (count // 2,), 0, 1 << 20) % (slack + 1)
    lengths = lengths.at[source_of].add(-moved).at[receiver].add(moved)
    labels = jnp.searchsorted(jnp.cumsum(lengths), jnp.arange(rows * top), side="right").astype(jnp.int32)
    table = labels.reshape(top, rows).T
    table = table[jax.random.permutation(jax.random.fold_in(own, 1), rows)]
    offset_by = jax.random.randint(jax.random.fold_in(own, 2), (rows, 1), 0, top)
    return jnp.take_along_axis(table, (jnp.arange(top)[None, :] + offset_by) % top, axis=1)


def load_shares(amount, total, reach, lean, full):
    portions = [(1 << 20) // math.isqrt(rank ** lean) + 1 for rank in range(1, amount + 1)]
    largest = reach if full else min(reach, max(-(-total // amount), total * portions[0] // sum(portions)))
    least = 1 if total - largest >= amount - 1 else 0
    holding, surplus = [largest] + [least] * (amount - 1), total - largest - least * (amount - 1)
    while surplus > 0:
        free = [i for i in range(1, amount) if holding[i] < largest] or [i for i in range(1, amount) if holding[i] < reach]
        whole, budget = sum([portions[i] for i in free]), surplus
        for i in free:
            extra = min(reach - holding[i], max(1, budget * portions[i] // whole), surplus)
            holding[i] = holding[i] + extra
            surplus = surplus - extra
    return np.array(holding)


def scatter_about(key, extent, deviation, limit, pieces=(), kind=jnp.bfloat16):
    entries = jax.random.normal(key, extent, jnp.float32) * deviation
    if len(pieces) > 0:
        entries = block_levels(key, extent, pieces, -0.22, 0.18) * entries
    return jnp.clip(entries, min=-limit, max=limit).astype(kind)


def setup_inputs(seed: int = 0) -> dict:
    splits = jax.random.split(jax.random.key(seed), 19)
    residual = draw_residual(jax.random.fold_in(splits[18], 71), 0)
    query_small = draw_query_small(jax.random.fold_in(splits[18], 71), 0)
    query_large = draw_query_large(jax.random.fold_in(splits[18], 71), 0)
    latent = draw_latent(jax.random.fold_in(splits[18], 71), 0)
    rotary_key = draw_rotary_key(jax.random.fold_in(splits[18], 71), 0)
    latent_gain = jnp.clip(1.0 + 0.18 * jax.random.normal(splits[5], (LATENT,), jnp.float32), 0.1, 1.9)
    small_keys = scatter_about(splits[6], (LATENT, HEADS_S * NOPE_S), LATENT ** -0.5, 0.25, ((1, 4),))
    small_values = scatter_about(splits[7], (LATENT, HEADS_S * V_S), LATENT ** -0.5, 0.25, ((1, 4),))
    large_keys = scatter_about(splits[8], (LATENT, HEADS_L * NOPE_L), LATENT ** -0.5, 0.25, ((1, 4),))
    large_values = scatter_about(splits[9], (LATENT, HEADS_L * V_L), LATENT ** -0.5, 0.25, ((1, 4),))
    small_output = scatter_about(splits[10], (HEADS_S * V_S, D), (HEADS_S * V_S + HEADS_L * V_L) ** -0.5, 0.21875, ((0, 4),))
    large_output = scatter_about(splits[11], (HEADS_L * V_L, D), (HEADS_S * V_S + HEADS_L * V_L) ** -0.5, 0.21875, ((0, 4),))
    ffn_gain = jnp.clip(1.0 + 0.18 * jax.random.normal(splits[12], (D,), jnp.float32), 0.1, 1.9)
    gate_weights = draw_gate_weights(jax.random.fold_in(splits[18], 71), 0)
    up_weights = draw_up_weights(jax.random.fold_in(splits[18], 71), 0)
    down_weights = scatter_about(splits[15], (EXPERTS, FF, D), (9 * FF) ** -0.5, 0.046875, ((0, 64), (1, 4)))
    routing_keys = jax.random.split(jax.random.fold_in(splits[16], 1), SEQ_LEN // TOK_DEV)
    routing_turns = jax.random.permutation(jax.random.fold_in(splits[16], 3), SEQ_LEN // TOK_DEV)
    routing = jax.vmap(lambda own, number: shared_out(jax.random.fold_in(splits[16], 2), own, number, TOK_DEV, EXPERTS, TOPK, CAP, 2))(routing_keys, routing_turns).reshape((SEQ_LEN, TOPK))
    route_weight = jnp.clip(jnp.exp(math.log(1.0) - 1.609438 * jax.random.uniform(splits[17], (SEQ_LEN, TOPK), jnp.float32) ** block_levels(splits[17], (SEQ_LEN, TOPK), ((0, 256),), -0.2, 0.2)), 0.2, 1.0)
    return {"residual": residual, "query_small": query_small, "query_large": query_large, "latent": latent, "rotary_key": rotary_key, "latent_gain": latent_gain, "small_keys": small_keys, "small_values": small_values, "large_keys": large_keys, "large_values": large_values, "small_output": small_output, "large_output": large_output, "ffn_gain": ffn_gain, "gate_weights": gate_weights, "up_weights": up_weights, "down_weights": down_weights, "routing": routing, "route_weight": route_weight}


eps = 1e-06
clamp_limit = 7.0
glu_alpha = 1.702
rope_base = 10000.0
masked_score = -1e+30

def rope_tables(row_count, first_pos):
    half_size = ROPE // 2
    frequencies = jnp.power(rope_base, -jnp.arange(half_size, dtype=jnp.float32) * (2.0 / ROPE))
    places = (first_pos + jnp.arange(row_count, dtype=jnp.int32)).astype(jnp.float32)
    angles = places[:, None] * frequencies[None, :]
    return (jnp.cos(angles), jnp.sin(angles))

def rotate(values_in, cos_vals, sin_vals):
    front_half, back_half = jnp.split(values_in, 2, axis=-1)
    return jnp.concatenate([front_half * cos_vals - back_half * sin_vals, back_half * cos_vals + front_half * sin_vals], axis=-1)

def rms_scaled(values_in, gain):
    widened = values_in.astype(jnp.float32)
    return widened * lax.rsqrt(lax.optimization_barrier(jnp.mean(widened * widened, axis=-1, keepdims=True)) + eps) * gain

def turn_queries(query, nope, cos_vals, sin_vals):
    width = nope + ROPE
    shaped = query.reshape(query.shape[0], query.shape[1] // width, width)
    turned = rotate(shaped[:, :, nope:].astype(jnp.float32), cos_vals[:, None, :], sin_vals[:, None, :])
    return jnp.concatenate([shaped[:, :, :nope], turned.astype(jnp.bfloat16)], axis=2)

def clamped(gate_pre, up_pre):
    limited = jnp.minimum(gate_pre, clamp_limit)
    linear = jnp.clip(up_pre, -clamp_limit, clamp_limit)
    return limited * jax.nn.sigmoid(glu_alpha * limited) * (linear + 1.0)

def attend_group(query, keys_in, values_in, rotary, nope):
    seq_rows = query.shape[0]
    head_count = query.shape[1]
    key_heads = keys_in.reshape(seq_rows, head_count, nope).astype(jnp.float32)
    value_heads = values_in.reshape(seq_rows, head_count, -1).astype(jnp.float32)
    rotary_wide = rotary.astype(jnp.float32)
    block_rows = math.gcd(seq_rows, 512)
    blocks = query.reshape(seq_rows // block_rows, block_rows, head_count, nope + ROPE)
    key_pos = jnp.arange(seq_rows, dtype=jnp.int32)

    def one_block(inputs):
        query_block, block_index = inputs
        query_wide = query_block.astype(jnp.float32)
        scores = jnp.einsum('qhd,khd->hqk', query_wide[:, :, :nope], key_heads)
        scores = scores + jnp.einsum('qhd,kd->hqk', query_wide[:, :, nope:], rotary_wide)
        query_pos = block_index * block_rows + jnp.arange(block_rows, dtype=jnp.int32)
        allowed = key_pos[None, :] <= query_pos[:, None]
        scores = jnp.where(allowed[None], scores * (nope + ROPE) ** (-0.5), masked_score)
        top_score = lax.optimization_barrier(jnp.max(scores, axis=2, keepdims=True))
        weights = jnp.exp(scores - top_score)
        weight_sum = lax.optimization_barrier(jnp.sum(weights, axis=2))
        rounded = lax.optimization_barrier(weights.astype(jnp.bfloat16)).astype(jnp.float32)
        mixed = jnp.einsum('hqk,khd->qhd', rounded, value_heads)
        return (mixed / weight_sum.T[:, :, None]).reshape(block_rows, -1).astype(jnp.bfloat16)
    outputs = lax.map(one_block, (blocks, jnp.arange(seq_rows // block_rows, dtype=jnp.int32)))
    return outputs.reshape(seq_rows, -1)

def expert_outputs(normed, routing, gate_weights, up_weights, down_weights):
    device_count = N_SP * N_TP
    assigned = routing.reshape(device_count, TOK_DEV * TOPK)
    onehot = (assigned[:, :, None] == jnp.arange(EXPERTS, dtype=jnp.int32)[None, None, :]).astype(jnp.int32)
    slot_index = lax.optimization_barrier(jnp.sum((jnp.cumsum(onehot, axis=1) - onehot) * onehot, axis=2))
    width_all = device_count * CAP
    places = assigned * width_all + jnp.arange(device_count, dtype=jnp.int32)[:, None] * CAP + slot_index
    places = places.reshape(-1).astype(jnp.int32)
    slot_table = jnp.full((EXPERTS * width_all,), -1, jnp.int32)
    slot_table = slot_table.at[places].set(jnp.arange(places.shape[0], dtype=jnp.int32))
    slot_table = slot_table.reshape(EXPERTS, width_all)
    run_width = FF // N_TP

    def one_expert(inputs):
        index_row, gate_one, up_one, down_one = inputs
        rows_in = normed[jnp.maximum(index_row, 0) // TOPK]
        gate_pre = jnp.dot(rows_in, gate_one, preferred_element_type=jnp.float32)
        up_pre = jnp.dot(rows_in, up_one, preferred_element_type=jnp.float32)
        hidden = clamped(gate_pre, up_pre).astype(jnp.bfloat16)
        summed = jnp.zeros((rows_in.shape[0], D), jnp.float32)
        for group_index in range(N_TP):
            lower = group_index * run_width
            partial_sum = jnp.dot(hidden[:, lower:lower + run_width], down_one[lower:lower + run_width], preferred_element_type=jnp.float32)
            summed = summed + lax.optimization_barrier(partial_sum.astype(jnp.bfloat16)).astype(jnp.float32)
        return summed.astype(jnp.bfloat16)
    outputs = lax.map(one_expert, (slot_table, gate_weights, up_weights, down_weights))
    return outputs.reshape(-1, D)[places]

def reference(residual, query_small, query_large, latent, rotary_key, latent_gain, small_keys, small_values, large_keys, large_values, small_output, large_output, ffn_gain, gate_weights, up_weights, down_weights, routing, route_weight):
    seq_rows = latent.shape[0]
    cos_vals, sin_vals = rope_tables(seq_rows, 0)
    small_query = turn_queries(query_small, NOPE_S, cos_vals, sin_vals)
    large_query = turn_queries(query_large, NOPE_L, cos_vals, sin_vals)
    normed_latent = rms_scaled(latent, latent_gain).astype(jnp.bfloat16)
    projected = [jnp.dot(normed_latent, weight, preferred_element_type=jnp.float32).astype(jnp.bfloat16) for weight in (small_keys, small_values, large_keys, large_values)]
    rotary = rotate(rotary_key.astype(jnp.float32), cos_vals, sin_vals).astype(jnp.bfloat16)
    small_heads = attend_group(small_query, projected[0], projected[1], rotary, NOPE_S)
    large_heads = attend_group(large_query, projected[2], projected[3], rotary, NOPE_L)
    small_span = HEADS_S // N_TP * V_S
    large_span = HEADS_L // N_TP * V_L
    summed = jnp.zeros((seq_rows, D), jnp.float32)
    for group_index in range(N_TP):
        small_low = group_index * small_span
        large_low = group_index * large_span
        partial_sum = jnp.dot(small_heads[:, small_low:small_low + small_span], small_output[small_low:small_low + small_span], preferred_element_type=jnp.float32)
        partial_sum = partial_sum + jnp.dot(large_heads[:, large_low:large_low + large_span], large_output[large_low:large_low + large_span], preferred_element_type=jnp.float32)
        summed = summed + lax.optimization_barrier(partial_sum.astype(jnp.bfloat16)).astype(jnp.float32)
    attention = lax.optimization_barrier(summed.astype(jnp.bfloat16)).astype(jnp.float32)
    middle = lax.optimization_barrier((residual.astype(jnp.float32) + attention).astype(jnp.bfloat16))
    normed = rms_scaled(middle, ffn_gain).astype(jnp.bfloat16)
    picked = expert_outputs(normed, routing, gate_weights, up_weights, down_weights)
    mixed = lax.optimization_barrier(jnp.sum(route_weight[:, :, None] * picked.astype(jnp.float32).reshape(seq_rows, TOPK, D), axis=1))
    return (middle.astype(jnp.float32) + mixed).astype(jnp.bfloat16)
```

```python
import functools

import jax
import jax.numpy as jnp
import numpy as np
from jax import lax
from jax.experimental import pallas as pl
from jax.experimental.pallas import tpu as pltpu
from jax.sharding import Mesh
from jax.sharding import PartitionSpec as P

NZ, NX, NC, NY = 8, 4, 2, 4
NXC = NX * NC
ROWS = 128
TOK = 32
D = 2048
NOPE_S = 64
NOPE_L = 128
ROPE = 32
EXPERTS = 64
CAP = 2
SLOTS = EXPERTS * CAP
FF_LOCAL = 512
EPS = 1e-6
LIMIT = 7.0
ALPHA = 1.702
ROPE_BASE = 10000.0
MASKED = -float(2**99)
LOG2E = 1.4426950408889634
SCALE_S = (NOPE_S + ROPE) ** -0.5 * LOG2E
SCALE_L = (NOPE_L + ROPE) ** -0.5 * LOG2E

f32 = jnp.float32
bf16 = jnp.bfloat16


def rope_parts():
    freq = ROPE_BASE ** (-np.arange(ROPE // 2, dtype=np.float64) * (2.0 / ROPE))

    def table(places):
        angles = places[:, None].astype(np.float64) * freq[None, :]
        c, s = np.cos(angles), np.sin(angles)
        return np.concatenate([c, c, s, s], axis=1).astype(np.float32)

    return table(np.arange(64) * ROWS), table(np.arange(ROWS))


def vmem(n):
    return [pl.BlockSpec(memory_space=pltpu.VMEM) for _ in range(n)]


def smem():
    return pl.BlockSpec(memory_space=pltpu.SMEM)


def pre_kernel(
    place_ref, lat_ref, gain_ref, rk_ref, qs_ref, ql_ref, ks_w, vs_w, kl_w, vl_w,
    base_ref, row_ref, kv_ref, q_ref,
):
    block = (place_ref[0] * NX + place_ref[1]) * NC + place_ref[2]
    base = base_ref[pl.ds(block, 1), :]
    row = row_ref[...]
    cb, sb = base[:, :ROPE], base[:, ROPE:]
    cr, sr = row[:, :ROPE], row[:, ROPE:]
    cos = cr * cb - sr * sb
    sin = sr * cb + cr * sb
    lane = lax.broadcasted_iota(jnp.int32, (ROWS, ROPE), 1)
    sin = jnp.where(lane < ROPE // 2, -sin, sin)

    def turned(v):
        v = v.astype(f32)
        swapped = jnp.concatenate([v[:, ROPE // 2 :], v[:, : ROPE // 2]], axis=1)
        return (v * cos + swapped * sin).astype(bf16)

    lat = lat_ref[...].astype(f32)
    scale = lax.rsqrt(jnp.mean(lat * lat, axis=1, keepdims=True) + EPS)
    normed = (lat * scale * gain_ref[...]).astype(bf16)

    def proj(w_ref):
        return jnp.dot(normed, w_ref[...], preferred_element_type=f32).astype(bf16)

    kv_ref[0:128, :] = proj(kl_w)
    kv_ref[128:256, :] = proj(vl_w)
    kv_ref[256:384, :] = jnp.concatenate([proj(ks_w), proj(vs_w)], axis=1)
    rot = turned(rk_ref[...])
    kv_ref[384:416, :] = jnp.concatenate([rot[32 * i : 32 * i + 32] for i in range(4)], axis=1)
    ql = ql_ref[...]
    qs = qs_ref[...]
    q_ref[0:128, :] = ql[:, :NOPE_L]
    q_ref[128:256, :] = jnp.concatenate(
        [qs[:, :NOPE_S], turned(ql[:, NOPE_L:]), turned(qs[:, NOPE_S:])], axis=1
    )


def attn_kernel(
    place_ref, k0, k1, k2, k3, k4, k5, k6, k7a, k7b, q0, q1, q2, q3, r_ref, out_ref,
    kl, ks, vl, vs,
):
    z, x, c = place_ref[0], place_ref[1], place_ref[2]
    ones = jnp.ones((ROWS, 128), bf16)
    zero32 = jnp.zeros((ROWS, 32), bf16)
    zero64 = jnp.zeros((ROWS, 64), bf16)
    blocks = [(k, k, 256) for k in (k0, k1, k2, k3, k4, k5, k6)] + [(k7a, k7b, 0)]
    for j, (front, back, at) in enumerate(blocks):
        lo, hi = j * ROWS, (j + 1) * ROWS
        small = back[at : at + 128, :]
        packed = back[at + 128 : at + 160, :]
        rot = jnp.concatenate([packed[:, 32 * i : 32 * i + 32] for i in range(4)], axis=0)
        kl[lo:hi, 0:128] = front[0:128, :]
        kl[lo:hi, 128:256] = jnp.concatenate([zero64, rot, zero32], axis=1)
        ks[lo:hi, :] = jnp.concatenate([small[:, :64], zero32, rot], axis=1)
        vl[lo:hi, 0:128] = front[128:256, :]
        vl[lo:hi, 128:256] = ones
        vs[lo:hi, 0:128] = small
        vs[lo:hi, 128:256] = ones
    shifts = (0, 1, 7, 2, 6, 3, 5, 4)
    lane = lax.broadcasted_iota(jnp.int32, (1, 128), 1)
    own = (x * NC + c) * ROWS
    kpos = jnp.concatenate(
        [lax.rem(z + (NZ - s), NZ) * (NXC * ROWS) + own + lane for s in shifts], axis=1
    )
    row = lax.broadcasted_iota(jnp.int32, (2 * ROWS, 1), 0)
    lanes = lax.broadcasted_iota(jnp.int32, (2 * ROWS, 128), 1)
    for d, (shift, mine) in enumerate(((0, q0), (1, q1), (3, q2), (2, q3))):
        xq = lax.rem(x + (NX - shift), NX)
        b_mine = xq * NC + c
        b_other = xq * NC + (1 - c)
        q = jnp.concatenate(
            [
                jnp.concatenate([mine[0:128, :], mine[128:256, :]], axis=1),
                jnp.concatenate([r_ref[d, 0:128, :], r_ref[d, 128:256, :]], axis=1),
            ],
            axis=0,
        )
        qpos = z * (NXC * ROWS) + jnp.where(
            row < ROWS, b_mine * ROWS + row, b_other * ROWS + row - ROWS
        )
        allowed = kpos <= qpos

        def attend(query, keys, values, scale):
            s = lax.dot_general(
                query, keys[...], (((1,), (1,)), ((), ())), preferred_element_type=f32
            )
            s = jnp.where(allowed, s, MASKED)
            top = jnp.max(s, axis=1, keepdims=True).astype(bf16).astype(f32)
            w = jnp.exp2((s - top) * scale).astype(bf16)
            o = jnp.dot(w, values[...], preferred_element_type=f32)
            total = o[:, 128:129]
            return o[:, :128] / total, top, total

        o_l, m_l, t_l = attend(q, kl, vl, SCALE_L)
        o_s, m_s, t_s = attend(q[:, 128:256], ks, vs, SCALE_S)
        h_l = t_l.astype(bf16).astype(f32)
        h_s = t_s.astype(bf16).astype(f32)
        for i, v in enumerate((m_l, h_l, t_l - h_l, m_s, h_s, t_s - h_s)):
            o_s = jnp.where(lanes == i, v, o_s)
        o_l = o_l.astype(bf16)
        o_s = o_s.astype(bf16)
        for half, b in ((0, b_mine), (1, b_other)):
            for y in range(NY):
                lo = half * ROWS + y * TOK
                out_ref[b, y, 0:TOK, :] = o_l[lo : lo + TOK]
                out_ref[b, y, TOK : 2 * TOK, :] = o_s[lo : lo + TOK]


def mid_kernel(
    place_ref, parts_ref, w0, w1, w3, w2a, w2b, res_ref, gain_ref, routing_ref,
    disp_ref, mid_ref, pick_ref,
):
    y = place_ref[3]
    total = jnp.zeros((TOK, D), f32)
    for shift, weights in ((0, (w0, w0, 96)), (1, (w1, w1, 96)), (3, (w3, w3, 96)), (2, (w2a, w2b, 0))):
        ya = lax.rem(y + (NY - shift), NY)
        larges = [parts_ref[i, ya, 0:TOK, :].astype(f32) for i in range(NXC)]
        smalls = [parts_ref[i, ya, TOK : 2 * TOK, :].astype(f32) for i in range(NXC)]

        def mixed(values, at, scale):
            tops = [s[:, at : at + 1] for s in smalls]
            top = functools.reduce(jnp.maximum, tops)
            ws = [
                (s[:, at + 1 : at + 2] + s[:, at + 2 : at + 3]) * jnp.exp2((t - top) * scale)
                for s, t in zip(smalls, tops)
            ]
            inv = 1.0 / functools.reduce(jnp.add, ws)
            return functools.reduce(jnp.add, [v * (w * inv) for v, w in zip(values, ws)])

        large = mixed(larges, 0, SCALE_L).astype(bf16)
        small = mixed(smalls, 3, SCALE_S)[:, 64:128].astype(bf16)
        heads = jnp.concatenate([large, small], axis=1)
        first, second, at = weights
        partial = jnp.dot(heads[:, :96], first[0:96, :], preferred_element_type=f32)
        partial = partial + jnp.dot(
            heads[:, 96:192], second[at : at + 96, :], preferred_element_type=f32
        )
        total = total + partial.astype(bf16).astype(f32)
    attention = total.astype(bf16).astype(f32)
    middle = (res_ref[...].astype(f32) + attention).astype(bf16)
    mid_ref[...] = middle
    wide = middle.astype(f32)
    scale = lax.rsqrt(jnp.mean(wide * wide, axis=1, keepdims=True) + EPS)
    normed = (wide * scale * gain_ref[...]).astype(bf16)

    lane = lax.broadcasted_iota(jnp.int32, (TOK, SLOTS), 1)
    r = [routing_ref[:, k : k + 1] for k in range(2)]
    hit = [lane == rk for rk in r]
    named = jnp.where(hit[0] | hit[1], 1.0, 0.0)
    tri = jnp.where(
        lax.broadcasted_iota(jnp.int32, (TOK, TOK), 1)
        < lax.broadcasted_iota(jnp.int32, (TOK, TOK), 0),
        1.0,
        0.0,
    )
    earlier = jnp.dot(tri.astype(bf16), named.astype(bf16), preferred_element_type=f32)
    send = jnp.zeros((TOK, SLOTS), f32)
    for k in range(2):
        slot = jnp.sum(jnp.where(hit[k], earlier, 0.0), axis=1, keepdims=True)
        pick = jnp.where(lane == r[k] * CAP + slot.astype(jnp.int32), 1.0, 0.0)
        pick_ref[k] = pick.astype(bf16)
        send = send + pick
    disp_ref[...] = lax.dot_general(
        send.astype(bf16), normed, (((0,), (0,)), ((), ())), preferred_element_type=f32
    ).astype(bf16)


def ffn_kernel(*refs):
    count = (len(refs) - 3) // 2
    xs, (wg, wu, wd), outs = refs[:count], refs[count : count + 3], refs[count + 3 :]
    rows = jnp.concatenate([x[...] for x in xs], axis=0) if count > 1 else xs[0][...]
    gate = jnp.dot(rows, wg[...], preferred_element_type=f32)
    up = jnp.dot(rows, wu[...], preferred_element_type=f32)
    m = jnp.minimum(gate, LIMIT)
    linear = jnp.clip(up, -LIMIT, LIMIT) + 1.0
    hidden = (m * jax.nn.sigmoid(ALPHA * m) * linear).astype(bf16)
    out = jnp.dot(hidden, wd[...], preferred_element_type=f32).astype(bf16)
    at = 0
    for x, o in zip(xs, outs):
        o[...] = out[at : at + x.shape[0]]
        at += x.shape[0]


def end_kernel(mid_ref, pick_ref, ret_ref, weight_ref, out_ref):
    total = mid_ref[...].astype(f32)
    ret = ret_ref[...]
    mixed = weight_ref[:, 0:1] * jnp.dot(pick_ref[0], ret, preferred_element_type=f32)
    mixed = mixed + weight_ref[:, 1:2] * jnp.dot(pick_ref[1], ret, preferred_element_type=f32)
    out_ref[...] = (total + mixed).astype(bf16)


def call(kernel, in_specs, shapes, scratch=(), flops=0):
    many = len(shapes) > 1
    outs = [jax.ShapeDtypeStruct(s, d) for s, d in shapes]
    return pl.pallas_call(
        kernel,
        in_specs=in_specs,
        out_specs=vmem(len(outs)) if many else vmem(1)[0],
        out_shape=outs if many else outs[0],
        scratch_shapes=list(scratch),
        compiler_params=pltpu.CompilerParams(vmem_limit_bytes=56 * 2**20),
        cost_estimate=pl.CostEstimate(flops=flops, transcendentals=0, bytes_accessed=0)
        if flops
        else None,
    )


def shifted(a, axis, size, by):
    return lax.ppermute(a, axis, [(i, (i + by) % size) for i in range(size)])


def on_device(
    residual, query_small, query_large, latent, rotary_key, latent_gain,
    small_keys, small_values, large_keys, large_values, small_output, large_output,
    ffn_gain, gate_weights, up_weights, down_weights, routing, route_weight,
):
    place = jnp.stack([lax.axis_index(a) for a in ("z", "x", "c", "y")]).astype(jnp.int32)
    base, row = rope_parts()
    kv, q = call(
        pre_kernel, [smem()] + vmem(11), [((416, 128), bf16), ((256, 128), bf16)]
    )(
        place, latent, latent_gain[None, :], rotary_key, query_small, query_large,
        small_keys, small_values, large_keys, large_values, base, row,
    )

    plus = minus = kv
    blocks = [kv]
    for _ in range(3):
        plus = shifted(plus, "z", NZ, 1)
        minus = shifted(minus, "z", NZ, -1)
        blocks += [plus, minus]
    blocks += [shifted(plus[:256], "z", NZ, 1), shifted(minus[256:], "z", NZ, -1)]

    qx = [q] + [shifted(q, "x", NX, s) for s in (1, -1, 2)]
    qc = shifted(jnp.stack(qx), "c", NC, 1)

    wo = jnp.concatenate([large_output, small_output], axis=0)
    wo_p = shifted(wo, "y", NY, 1)
    wo_m = shifted(wo, "y", NY, -1)
    wo_a = shifted(wo_p[:96], "y", NY, 1)
    wo_b = shifted(wo_m[96:], "y", NY, -1)

    parts = call(
        attn_kernel,
        [smem()] + vmem(14),
        [((NXC, NY, 2 * TOK, 128), bf16)],
        scratch=[
            pltpu.VMEM((1024, 256), bf16),
            pltpu.VMEM((1024, 128), bf16),
            pltpu.VMEM((1024, 256), bf16),
            pltpu.VMEM((1024, 256), bf16),
        ],
    )(place, *blocks, *qx, qc)
    parts = lax.all_to_all(
        parts.reshape(NXC * NY * 2 * TOK, 128), ("x", "c", "y"), 0, 0, tiled=True
    ).reshape(NXC, NY, 2 * TOK, 128)

    disp, middle, pick = call(
        mid_kernel,
        [smem()] + vmem(9),
        [((SLOTS, D), bf16), ((TOK, D), bf16), ((2, TOK, SLOTS), bf16)],
    )(place, parts, wo, wo_p, wo_m, wo_a, wo_b, residual, ffn_gain[None, :], routing)

    sp = ("z", "x", "c")
    mine = lax.all_to_all(disp.reshape(EXPERTS, CAP, D), sp, 0, 0, tiled=True)
    mine = mine.reshape(SLOTS, D)

    half = SLOTS // 2
    x_a, x_b = mine[:half], mine[half:]
    weights = (gate_weights[0], up_weights[0], down_weights[0])

    def ffn(*pieces):
        return call(
            ffn_kernel,
            vmem(len(pieces) + 3),
            [(p.shape, bf16) for p in pieces],
        )(*pieces, *weights)

    p_a = shifted(x_a, "y", NY, 1)
    m_b = shifted(x_b, "y", NY, -1)
    p_b = shifted(x_b, "y", NY, 1)
    m_a = shifted(x_a, "y", NY, -1)
    o_a = shifted(p_a, "y", NY, 1)
    o_b = shifted(m_b, "y", NY, -1)
    r0_a, r0_b = ffn(x_a, x_b)
    r1_a, r1_b, r3_a, r3_b = ffn(p_a, p_b, m_a, m_b)
    r2_a, r2_b = ffn(o_a, o_b)

    from_m_b = shifted(r3_b, "y", NY, 1)
    from_p_a = shifted(r1_a, "y", NY, -1)
    t_a = shifted(r2_a, "y", NY, 1)
    t_b = shifted(r2_b, "y", NY, -1)
    r3_a = (r3_a.astype(f32) + t_a.astype(f32)).astype(bf16)
    r1_b = (r1_b.astype(f32) + t_b.astype(f32)).astype(bf16)
    from_m_a = shifted(r3_a, "y", NY, 1)
    from_p_b = shifted(r1_b, "y", NY, -1)
    done = jnp.concatenate(
        [
            r0_a.astype(f32) + from_m_a.astype(f32) + from_p_a.astype(f32),
            r0_b.astype(f32) + from_m_b.astype(f32) + from_p_b.astype(f32),
        ],
        axis=0,
    ).astype(bf16)
    ret = lax.all_to_all(done.reshape(EXPERTS, CAP, D), sp, 0, 0, tiled=True)
    return call(end_kernel, vmem(4), [((TOK, D), bf16)])(
        middle, pick, ret.reshape(SLOTS, D), route_weight
    )


def solution(mesh):
    fine = Mesh(mesh.devices.reshape(NZ, NX, NC, NY), ("z", "x", "c", "y"))
    sp = ("z", "x", "c")
    every = ("z", "x", "c", "y")
    return jax.shard_map(
        on_device,
        mesh=fine,
        in_specs=(
            P(every, None),
            P(sp, "y"),
            P(sp, "y"),
            P(sp, None),
            P(sp, None),
            P(),
            P(None, "y"),
            P(None, "y"),
            P(None, "y"),
            P(None, "y"),
            P("y", None),
            P("y", None),
            P(),
            P(sp, None, "y"),
            P(sp, None, "y"),
            P(sp, "y", None),
            P(every, None),
            P(every, None),
        ),
        out_specs=P(every, None),
        check_vma=False,
    )
```

```python
import functools

import jax
import jax.numpy as jnp
import numpy as np
from jax import lax
from jax.experimental import pallas as pl
from jax.experimental.pallas import tpu as pltpu
from jax.sharding import Mesh
from jax.sharding import PartitionSpec as P

NZ, NX, NC, NY = 8, 4, 2, 4
NXC = NX * NC
ROWS = 128
TOK = 32
D = 2048
NOPE_S = 64
NOPE_L = 128
ROPE = 32
EXPERTS = 64
CAP = 2
SLOTS = EXPERTS * CAP
FF_LOCAL = 512
EPS = 1e-6
LIMIT = 7.0
ALPHA = 1.702
ROPE_BASE = 10000.0
MASKED = -float(2**99)
LOG2E = 1.4426950408889634
SCALE_S = (NOPE_S + ROPE) ** -0.5 * LOG2E
SCALE_L = (NOPE_L + ROPE) ** -0.5 * LOG2E

f32 = jnp.float32
bf16 = jnp.bfloat16


def rope_parts():
    freq = ROPE_BASE ** (-np.arange(ROPE // 2, dtype=np.float64) * (2.0 / ROPE))

    def table(places):
        angles = places[:, None].astype(np.float64) * freq[None, :]
        c, s = np.cos(angles), np.sin(angles)
        return np.concatenate([c, c, s, s], axis=1).astype(np.float32)

    return table(np.arange(64) * ROWS), np.ascontiguousarray(table(np.arange(ROWS)).T)


def vmem(n):
    return [pl.BlockSpec(memory_space=pltpu.VMEM) for _ in range(n)]


def smem():
    return pl.BlockSpec(memory_space=pltpu.SMEM)


def column(row):
    n = row.shape[1]
    same = lax.broadcasted_iota(jnp.int32, (n, n), 0) == lax.broadcasted_iota(
        jnp.int32, (n, n), 1
    )
    return jnp.sum(jnp.where(same, row, 0.0), axis=1, keepdims=True)


def pre_kernel(
    place_ref, lat_ref, gain_ref, rk_ref, qs_ref, ql_ref, ks_w, vs_w, kl_w, vl_w,
    base_ref, row_ref, lo_ref, so_ref, kv_ref, q_ref, wo_ref,
):
    block = (place_ref[0] * NX + place_ref[1]) * NC + place_ref[2]
    base = column(base_ref[pl.ds(block, 1), :])
    cb, sb = base[:ROPE], base[ROPE:]
    cr, sr = row_ref[:ROPE], row_ref[ROPE:]
    cos = cr * cb - sr * sb
    sin = sr * cb + cr * sb
    at = lax.broadcasted_iota(jnp.int32, (ROPE, ROWS), 0)
    sin = jnp.where(at < ROPE // 2, -sin, sin)

    def turned(v):
        v = v.astype(f32)
        swapped = jnp.concatenate([v[ROPE // 2 :], v[: ROPE // 2]], axis=0)
        return v * cos + swapped * sin

    lat = lat_ref[...].astype(f32)
    scale = lax.rsqrt(jnp.mean(lat * lat, axis=1, keepdims=True) + EPS)
    normed = (lat * scale * gain_ref[...]).astype(bf16)
    across = (((1,), (1,)), ((), ()))

    kv_ref[0, 0:128, :] = jnp.dot(normed, kl_w[...], preferred_element_type=f32).T.astype(bf16)
    kv_ref[0, 128:256, :] = jnp.dot(normed, vl_w[...], preferred_element_type=f32).astype(bf16)
    kv_ref[0, 256:320, :] = lax.dot_general(
        ks_w[...], normed, across, preferred_element_type=f32
    ).astype(bf16)
    kv_ref[0, 320:352, :] = turned(rk_ref[...]).astype(bf16)
    kv_ref[0, 352:416, :] = lax.dot_general(
        vs_w[...], normed, across, preferred_element_type=f32
    ).astype(bf16)
    for j in range(1, NZ):
        kv_ref[j] = kv_ref[0]
    q_ref[0:128, :] = ql_ref[0:NOPE_L, :].astype(f32).T.astype(bf16)
    mixed = jnp.concatenate(
        [qs_ref[0:NOPE_S, :].astype(f32), turned(ql_ref[NOPE_L:, :]), turned(qs_ref[NOPE_S:, :])],
        axis=0,
    )
    q_ref[128:256, :] = mixed.T.astype(bf16)
    wo_ref[0:128, :] = lo_ref[...]
    wo_ref[128:192, :] = so_ref[...]


def attn_kernel(place_ref, kv_ref, q0, q1, q2, q3, r_ref, out_ref, kl, ks, vl, vs):
    z, x, c = place_ref[0], place_ref[1], place_ref[2]
    kl[128:192, :] = jnp.zeros((64, 1024), bf16)
    kl[224:256, :] = jnp.zeros((32, 1024), bf16)
    ks[64:96, :] = jnp.zeros((32, 1024), bf16)
    vl[:, 128:256] = jnp.ones((1024, 128), bf16)
    vs[0:64, :] = jnp.ones((64, 1024), bf16)
    for j in range(NZ):
        lo, hi = j * ROWS, (j + 1) * ROWS
        rot = kv_ref[j, 320:352, :]
        kl[0:128, lo:hi] = kv_ref[j, 0:128, :]
        kl[192:224, lo:hi] = rot
        ks[0:64, lo:hi] = kv_ref[j, 256:320, :]
        ks[96:128, lo:hi] = rot
        vl[lo:hi, 0:128] = kv_ref[j, 128:256, :]
        vs[64:128, lo:hi] = kv_ref[j, 352:416, :]
    key = lax.broadcasted_iota(jnp.int32, (1, NZ * ROWS), 1)
    kpos = (key // ROWS) * (NXC * ROWS) + (x * NC + c) * ROWS + lax.rem(key, ROWS)
    row = lax.broadcasted_iota(jnp.int32, (2 * ROWS, 1), 0)
    lanes = lax.broadcasted_iota(jnp.int32, (2 * ROWS, 128), 1)
    for d, (shift, mine) in enumerate(((0, q0), (1, q1), (3, q2), (2, q3))):
        xq = lax.rem(x + (NX - shift), NX)
        b_mine = xq * NC + c
        b_other = xq * NC + (1 - c)
        q = jnp.concatenate(
            [
                jnp.concatenate([mine[0:128, :], mine[128:256, :]], axis=1),
                jnp.concatenate([r_ref[d, 0:128, :], r_ref[d, 128:256, :]], axis=1),
            ],
            axis=0,
        )
        qpos = z * (NXC * ROWS) + jnp.where(
            row < ROWS, b_mine * ROWS + row, b_other * ROWS + row - ROWS
        )
        allowed = kpos <= qpos

        def attend(query, keys, values, contract, scale, at):
            s = jnp.dot(query, keys[...], preferred_element_type=f32)
            s = jnp.where(allowed, s, MASKED)
            top = jnp.max(s, axis=1, keepdims=True).astype(bf16).astype(f32)
            w = jnp.exp2((s - top) * scale).astype(bf16)
            o = lax.dot_general(
                w, values[...], (((1,), (contract,)), ((), ())), preferred_element_type=f32
            )
            total = o[:, at : at + 1]
            return o[:, :128] / total, top, total

        o_l, m_l, t_l = attend(q, kl, vl, 0, SCALE_L, 128)
        o_s, m_s, t_s = attend(q[:, 128:256], ks, vs, 1, SCALE_S, 0)
        h_l = t_l.astype(bf16).astype(f32)
        h_s = t_s.astype(bf16).astype(f32)
        for i, v in enumerate((m_l, h_l, t_l - h_l, m_s, h_s, t_s - h_s)):
            o_s = jnp.where(lanes == i, v, o_s)
        o_l = o_l.astype(bf16)
        o_s = o_s.astype(bf16)
        for half, b in ((0, b_mine), (1, b_other)):
            for y in range(NY):
                lo = half * ROWS + y * TOK
                out_ref[b, y, 0:TOK, :] = o_l[lo : lo + TOK]
                out_ref[b, y, TOK : 2 * TOK, :] = o_s[lo : lo + TOK]


def mid_kernel(
    place_ref, parts_ref, w0, w1, w3, w2a, w2b, res_ref, gain_ref, routing_ref,
    disp_ref, mid_ref, pick_ref,
):
    y = place_ref[3]
    total = jnp.zeros((TOK, D), f32)
    for shift, weights in ((0, (w0, w0, 96)), (1, (w1, w1, 96)), (3, (w3, w3, 96)), (2, (w2a, w2b, 0))):
        ya = lax.rem(y + (NY - shift), NY)
        larges = [parts_ref[i, ya, 0:TOK, :].astype(f32) for i in range(NXC)]
        smalls = [parts_ref[i, ya, TOK : 2 * TOK, :].astype(f32) for i in range(NXC)]

        def mixed(values, at, scale):
            tops = [s[:, at : at + 1] for s in smalls]
            top = functools.reduce(jnp.maximum, tops)
            ws = [
                (s[:, at + 1 : at + 2] + s[:, at + 2 : at + 3]) * jnp.exp2((t - top) * scale)
                for s, t in zip(smalls, tops)
            ]
            inv = 1.0 / functools.reduce(jnp.add, ws)
            return functools.reduce(jnp.add, [v * (w * inv) for v, w in zip(values, ws)])

        large = mixed(larges, 0, SCALE_L).astype(bf16)
        small = mixed(smalls, 3, SCALE_S)[:, 64:128].astype(bf16)
        heads = jnp.concatenate([large, small], axis=1)
        first, second, at = weights
        partial = jnp.dot(heads[:, :96], first[0:96, :], preferred_element_type=f32)
        partial = partial + jnp.dot(
            heads[:, 96:192], second[at : at + 96, :], preferred_element_type=f32
        )
        total = total + partial.astype(bf16).astype(f32)
    attention = total.astype(bf16).astype(f32)
    middle = (res_ref[...].astype(f32) + attention).astype(bf16)
    mid_ref[...] = middle
    wide = middle.astype(f32)
    scale = lax.rsqrt(jnp.mean(wide * wide, axis=1, keepdims=True) + EPS)
    normed = (wide * scale * gain_ref[...]).astype(bf16)

    lane = lax.broadcasted_iota(jnp.int32, (TOK, SLOTS), 1)
    named_by = routing_ref[...].astype(f32)
    r = [column(named_by[k : k + 1, :]).astype(jnp.int32) for k in range(2)]
    hit = [lane == rk for rk in r]
    named = jnp.where(hit[0] | hit[1], 1.0, 0.0)
    tri = jnp.where(
        lax.broadcasted_iota(jnp.int32, (TOK, TOK), 1)
        < lax.broadcasted_iota(jnp.int32, (TOK, TOK), 0),
        1.0,
        0.0,
    )
    earlier = jnp.dot(tri.astype(bf16), named.astype(bf16), preferred_element_type=f32)
    send = jnp.zeros((TOK, SLOTS), f32)
    for k in range(2):
        slot = jnp.sum(jnp.where(hit[k], earlier, 0.0), axis=1, keepdims=True)
        pick = jnp.where(lane == r[k] * CAP + slot.astype(jnp.int32), 1.0, 0.0)
        pick_ref[k] = pick.astype(bf16)
        send = send + pick
    disp_ref[...] = lax.dot_general(
        send.astype(bf16), normed, (((0,), (0,)), ((), ())), preferred_element_type=f32
    ).astype(bf16)


def load_kernel(a, b, c, out_a, out_b, out_c, sems):
    copies = [
        pltpu.make_async_copy(src, dst, sems.at[i])
        for i, (src, dst) in enumerate(((a, out_a), (b, out_b), (c, out_c)))
    ]
    for copy in copies:
        copy.start()
    for copy in copies:
        copy.wait()


def ffn_kernel(*refs):
    count = (len(refs) - 3) // 2
    xs, (wg, wu, wd), outs = refs[:count], refs[count : count + 3], refs[count + 3 :]
    rows = jnp.concatenate([x[...] for x in xs], axis=0) if count > 1 else xs[0][...]
    gate = jnp.dot(rows, wg[...], preferred_element_type=f32)
    up = jnp.dot(rows, wu[...], preferred_element_type=f32)
    m = jnp.minimum(gate, LIMIT)
    linear = jnp.clip(up, -LIMIT, LIMIT) + 1.0
    hidden = (m * jax.nn.sigmoid(ALPHA * m) * linear).astype(bf16)
    out = jnp.dot(hidden, wd[...], preferred_element_type=f32).astype(bf16)
    at = 0
    for x, o in zip(xs, outs):
        o[...] = out[at : at + x.shape[0]]
        at += x.shape[0]


def end_kernel(mid_ref, pick_ref, ret_ref, weight_ref, out_ref):
    total = mid_ref[...].astype(f32)
    ret = ret_ref[...]
    weight = weight_ref[...]
    mixed = column(weight[0:1, :]) * jnp.dot(pick_ref[0], ret, preferred_element_type=f32)
    mixed = mixed + column(weight[1:2, :]) * jnp.dot(
        pick_ref[1], ret, preferred_element_type=f32
    )
    out_ref[...] = (total + mixed).astype(bf16)


def call(kernel, in_specs, shapes, scratch=(), flops=0, mib=16):
    many = len(shapes) > 1
    outs = [jax.ShapeDtypeStruct(s, d) for s, d in shapes]
    return pl.pallas_call(
        kernel,
        in_specs=in_specs,
        out_specs=vmem(len(outs)) if many else vmem(1)[0],
        out_shape=outs if many else outs[0],
        scratch_shapes=list(scratch),
        compiler_params=pltpu.CompilerParams(vmem_limit_bytes=mib * 2**20),
        cost_estimate=pl.CostEstimate(flops=flops, transcendentals=0, bytes_accessed=0)
        if flops
        else None,
    )


def shifted(a, axis, size, by):
    return lax.ppermute(a, axis, [(i, (i + by) % size) for i in range(size)])


def layer(
    residual, query_small, query_large, latent, rotary_key, latent_gain,
    small_keys, small_values, large_keys, large_values, small_output, large_output,
    ffn_gain, gate_weights, up_weights, down_weights, routing, route_weight,
):
    place = jnp.stack([lax.axis_index(a) for a in ("z", "x", "c", "y")]).astype(jnp.int32)
    base, row = rope_parts()
    kv, q, wo = call(
        pre_kernel,
        [smem()] + vmem(13),
        [((NZ, 416, 128), bf16), ((256, 128), bf16), ((192, D), bf16)],
        flops=10**9,
        mib=63,
    )(
        place, latent, latent_gain[None, :], rotary_key.T, query_small.T, query_large.T,
        small_keys.T, small_values.T, large_keys, large_values, base, row,
        large_output, small_output,
    )

    kvs = lax.all_to_all(kv, "z", 0, 0, tiled=True)

    qx = [q]
    for by in (1, -1, 2):
        qx.append(shifted(q, "x", NX, by))
    qc = shifted(jnp.stack(qx), "c", NC, 1)

    wo_p = shifted(wo, "y", NY, 1)
    wo_m = shifted(wo, "y", NY, -1)
    kvs, wo_p, wo_m = lax.optimization_barrier((kvs, wo_p, wo_m))
    wo_a = shifted(wo_p[:96], "y", NY, 1)
    wo_b = shifted(wo_m[96:], "y", NY, -1)

    attend = call(
        attn_kernel,
        [smem()] + vmem(6),
        [((NXC, NY, 2 * TOK, 128), bf16)],
        scratch=[
            pltpu.VMEM((256, 1024), bf16),
            pltpu.VMEM((128, 1024), bf16),
            pltpu.VMEM((1024, 256), bf16),
            pltpu.VMEM((128, 1024), bf16),
        ],
        flops=3 * 10**9,
        mib=24,
    )
    parts = attend(place, kvs, *qx, qc)
    parts = lax.all_to_all(
        parts.reshape(NXC * NY * 2 * TOK, 128), ("x", "c", "y"), 0, 0, tiled=True
    ).reshape(NXC, NY, 2 * TOK, 128)

    disp, middle, pick = call(
        mid_kernel,
        [smem()] + vmem(9),
        [((SLOTS, D), bf16), ((TOK, D), bf16), ((2, TOK, SLOTS), bf16)],
        flops=2 * 10**9,
        mib=63,
    )(place, parts, wo, wo_p, wo_m, wo_a, wo_b, residual, ffn_gain[None, :], routing.T)

    sp = ("z", "x", "c")
    mine = lax.all_to_all(disp.reshape(EXPERTS, CAP, D), sp, 0, 0, tiled=True)
    mine = mine.reshape(SLOTS, D)

    half = SLOTS // 2
    x_a, x_b = mine[:half], mine[half:]
    weights = call(
        load_kernel,
        [pl.BlockSpec(memory_space=pltpu.HBM) for _ in range(3)],
        [((D, FF_LOCAL), bf16), ((D, FF_LOCAL), bf16), ((FF_LOCAL, D), bf16)],
        scratch=[pltpu.SemaphoreType.DMA((3,))],
        flops=10**9,
        mib=8,
    )(gate_weights[0], up_weights[0], down_weights[0])

    def ffn(*pieces):
        return call(
            ffn_kernel,
            vmem(len(pieces) + 3),
            [(p.shape, bf16) for p in pieces],
            flops=3 * 10**9,
            mib=28,
        )(*pieces, *weights)

    p_a = shifted(x_a, "y", NY, 1)
    m_b = shifted(x_b, "y", NY, -1)
    p_b = shifted(x_b, "y", NY, 1)
    m_a = shifted(x_a, "y", NY, -1)
    o_a = shifted(p_a, "y", NY, 1)
    o_b = shifted(m_b, "y", NY, -1)
    r0_a, r0_b, r1_a, r1_b, r3_a, r3_b = ffn(x_a, x_b, p_a, p_b, m_a, m_b)
    r2_a, r2_b = ffn(o_a, o_b)

    from_m_b = shifted(r3_b, "y", NY, 1)
    from_p_a = shifted(r1_a, "y", NY, -1)
    t_a = shifted(r2_a, "y", NY, 1)
    t_b = shifted(r2_b, "y", NY, -1)
    r3_a = (r3_a.astype(f32) + t_a.astype(f32)).astype(bf16)
    r1_b = (r1_b.astype(f32) + t_b.astype(f32)).astype(bf16)
    from_m_a = shifted(r3_a, "y", NY, 1)
    from_p_b = shifted(r1_b, "y", NY, -1)
    done = jnp.concatenate(
        [
            r0_a.astype(f32) + from_m_a.astype(f32) + from_p_a.astype(f32),
            r0_b.astype(f32) + from_m_b.astype(f32) + from_p_b.astype(f32),
        ],
        axis=0,
    ).astype(bf16)
    ret = lax.all_to_all(done.reshape(EXPERTS, CAP, D), sp, 0, 0, tiled=True)
    return call(end_kernel, vmem(4), [((TOK, D), bf16)])(
        middle, pick, ret.reshape(SLOTS, D), route_weight.T
    )


def solution(mesh):
    fine = Mesh(mesh.devices.reshape(NZ, NX, NC, NY), ("z", "x", "c", "y"))
    sp = ("z", "x", "c")
    every = ("z", "x", "c", "y")
    return jax.shard_map(
        layer,
        mesh=fine,
        in_specs=(
            P(every, None),
            P(sp, "y"),
            P(sp, "y"),
            P(sp, None),
            P(sp, None),
            P(),
            P(None, "y"),
            P(None, "y"),
            P(None, "y"),
            P(None, "y"),
            P("y", None),
            P("y", None),
            P(),
            P(sp, None, "y"),
            P(sp, None, "y"),
            P(sp, "y", None),
            P(every, None),
            P(every, None),
        ),
        out_specs=P(every, None),
        check_vma=False,
    )
```

```python
import functools

import jax
import jax.numpy as jnp
import numpy as np
from jax import lax
from jax.experimental import pallas as pl
from jax.experimental.pallas import tpu as pltpu
from jax.sharding import Mesh
from jax.sharding import PartitionSpec as P

NZ, NX, NC, NY = 8, 4, 2, 4
NXC = NX * NC
ROWS = 128
TOK = 32
D = 2048
NOPE_S = 64
NOPE_L = 128
ROPE = 32
EXPERTS = 64
CAP = 2
SLOTS = EXPERTS * CAP
FF_LOCAL = 512
EPS = 1e-6
LIMIT = 7.0
ALPHA = 1.702
ROPE_BASE = 10000.0
MASKED = -float(2**99)
LOG2E = 1.4426950408889634
SCALE_S = (NOPE_S + ROPE) ** -0.5 * LOG2E
SCALE_L = (NOPE_L + ROPE) ** -0.5 * LOG2E


f32 = jnp.float32
bf16 = jnp.bfloat16


def rope_parts():
    freq = ROPE_BASE ** (-np.arange(ROPE // 2, dtype=np.float64) * (2.0 / ROPE))

    def table(places):
        angles = places[:, None].astype(np.float64) * freq[None, :]
        c, s = np.cos(angles), np.sin(angles)
        return np.concatenate([c, c, s, s], axis=1).astype(np.float32)

    return table(np.arange(64) * ROWS), np.ascontiguousarray(table(np.arange(ROWS)).T)


def vmem(n):
    return [pl.BlockSpec(memory_space=pltpu.VMEM) for _ in range(n)]


def smem():
    return pl.BlockSpec(memory_space=pltpu.SMEM)


def column(row):
    n = row.shape[1]
    same = lax.broadcasted_iota(jnp.int32, (n, n), 0) == lax.broadcasted_iota(
        jnp.int32, (n, n), 1
    )
    return jnp.sum(jnp.where(same, row, 0.0), axis=1, keepdims=True)


def pre_kernel(
    place_ref, lat_ref, gain_ref, rk_ref, qs_ref, ql_ref, ks_w, vs_w, kl_w, vl_w,
    base_ref, row_ref, lo_ref, so_ref, kv_ref, q_ref, top_ref, low_ref,
):
    block = (place_ref[0] * NX + place_ref[1]) * NC + place_ref[2]
    base = column(base_ref[pl.ds(block, 1), :])
    cb, sb = base[:ROPE], base[ROPE:]
    cr, sr = row_ref[:ROPE], row_ref[ROPE:]
    cos = cr * cb - sr * sb
    sin = sr * cb + cr * sb
    at = lax.broadcasted_iota(jnp.int32, (ROPE, ROWS), 0)
    sin = jnp.where(at < ROPE // 2, -sin, sin)

    def turned(v):
        v = v.astype(f32)
        swapped = jnp.concatenate([v[ROPE // 2 :], v[: ROPE // 2]], axis=0)
        return v * cos + swapped * sin

    lat = lat_ref[...].astype(f32)
    scale = lax.rsqrt(jnp.mean(lat * lat, axis=1, keepdims=True) + EPS)
    normed = (lat * scale * gain_ref[...]).astype(bf16)
    across = (((1,), (1,)), ((), ()))

    kv_ref[0, 0:128, :] = jnp.dot(normed, kl_w[...], preferred_element_type=f32).T.astype(bf16)
    kv_ref[0, 128:256, :] = jnp.dot(normed, vl_w[...], preferred_element_type=f32).astype(bf16)
    kv_ref[0, 256:320, :] = lax.dot_general(
        ks_w[...], normed, across, preferred_element_type=f32
    ).astype(bf16)
    kv_ref[0, 320:352, :] = turned(rk_ref[...]).astype(bf16)
    kv_ref[0, 352:416, :] = lax.dot_general(
        vs_w[...], normed, across, preferred_element_type=f32
    ).astype(bf16)
    for j in range(1, NZ):
        kv_ref[j] = kv_ref[0]
    q_ref[0:128, :] = ql_ref[0:NOPE_L, :].astype(f32).T.astype(bf16)
    mixed = jnp.concatenate(
        [qs_ref[0:NOPE_S, :].astype(f32), turned(ql_ref[NOPE_L:, :]), turned(qs_ref[NOPE_S:, :])],
        axis=0,
    )
    q_ref[128:256, :] = mixed.T.astype(bf16)
    top_ref[...] = lo_ref[0:96, :]
    low_ref[0:32, :] = lo_ref[96:128, :]
    low_ref[32:96, :] = so_ref[...]


def attn_kernel(other, place_ref, kv_ref, *refs):
    queries, (out_ref, kl, ks, vl, vs) = refs[:-5], refs[-5:]
    z, x, c = place_ref[0], place_ref[1], place_ref[2]
    kl[128:192, :] = jnp.zeros((64, 1024), bf16)
    kl[224:256, :] = jnp.zeros((32, 1024), bf16)
    ks[64:96, :] = jnp.zeros((32, 1024), bf16)
    vl[:, 128:256] = jnp.ones((1024, 128), bf16)
    vs[0:64, :] = jnp.ones((64, 1024), bf16)
    for j in range(NZ):
        lo, hi = j * ROWS, (j + 1) * ROWS
        rot = kv_ref[j, 320:352, :]
        kl[0:128, lo:hi] = kv_ref[j, 0:128, :]
        kl[192:224, lo:hi] = rot
        ks[0:64, lo:hi] = kv_ref[j, 256:320, :]
        ks[96:128, lo:hi] = rot
        vl[lo:hi, 0:128] = kv_ref[j, 128:256, :]
        vs[64:128, lo:hi] = kv_ref[j, 352:416, :]
    key = lax.broadcasted_iota(jnp.int32, (1, NZ * ROWS), 1)
    kpos = (key // ROWS) * (NXC * ROWS) + (x * NC + c) * ROWS + lax.rem(key, ROWS)
    row = lax.broadcasted_iota(jnp.int32, (2 * ROWS, 1), 0)
    lanes = lax.broadcasted_iota(jnp.int32, (2 * ROWS, 128), 1)
    core = 1 - c if other else c
    for d in (0, 2):
        block = [queries[0][d + i] if other else queries[d + i][...] for i in range(2)]
        xq = [lax.rem(x + (NX - s), NX) for s in ((0, 1) if d == 0 else (3, 2))]
        q = jnp.concatenate(
            [jnp.concatenate([b[0:128, :], b[128:256, :]], axis=1) for b in block], axis=0
        )
        qpos = z * (NXC * ROWS) + jnp.where(
            row < ROWS,
            (xq[0] * NC + core) * ROWS + row,
            (xq[1] * NC + core) * ROWS + row - ROWS,
        )
        allowed = kpos <= qpos

        def attend(query, keys, values, contract, scale, at):
            s = jnp.dot(query, keys[...], preferred_element_type=f32)
            s = jnp.where(allowed, s, MASKED)
            top = jnp.max(s, axis=1, keepdims=True).astype(bf16).astype(f32)
            w = jnp.exp2((s - top) * scale).astype(bf16)
            o = lax.dot_general(
                w, values[...], (((1,), (contract,)), ((), ())), preferred_element_type=f32
            )
            total = o[:, at : at + 1]
            return o[:, :128] / total, top, total

        o_l, m_l, t_l = attend(q, kl, vl, 0, SCALE_L, 128)
        o_s, m_s, t_s = attend(q[:, 128:256], ks, vs, 1, SCALE_S, 0)
        h_l = t_l.astype(bf16).astype(f32)
        h_s = t_s.astype(bf16).astype(f32)
        for i, v in enumerate((m_l, h_l, t_l - h_l, m_s, h_s, t_s - h_s)):
            o_s = jnp.where(lanes == i, v, o_s)
        o_l = o_l.astype(bf16)
        o_s = o_s.astype(bf16)
        for half in range(2):
            for y in range(NY):
                lo = half * ROWS + y * TOK
                out_ref[xq[half], y, 0:TOK, :] = o_l[lo : lo + TOK]
                out_ref[xq[half], y, TOK : 2 * TOK, :] = o_s[lo : lo + TOK]


def merge_kernel(a_ref, b_ref, out_ref):
    rows = NX * NY * TOK
    ref = [r[...].astype(f32) for r in (a_ref, b_ref)]
    large = [r[:, :TOK].reshape(rows, 128) for r in ref]
    small = [r[:, TOK:].reshape(rows, 128) for r in ref]
    lanes = lax.broadcasted_iota(jnp.int32, (rows, 128), 1)
    outs = []
    stats = []
    for at, scale, values in ((0, SCALE_L, large), (3, SCALE_S, small)):
        tops = [s[:, at : at + 1] for s in small]
        top = jnp.maximum(tops[0], tops[1])
        ws = [
            (s[:, at + 1 : at + 2] + s[:, at + 2 : at + 3]) * jnp.exp2((t - top) * scale)
            for s, t in zip(small, tops)
        ]
        total = ws[0] + ws[1]
        outs.append(values[0] * (ws[0] / total) + values[1] * (ws[1] / total))
        high = total.astype(bf16).astype(f32)
        stats += [top, high, total - high]
    for i, v in enumerate(stats):
        outs[1] = jnp.where(lanes == i, v, outs[1])
    out_ref[:, :TOK] = outs[0].astype(bf16).reshape(NX * NY, TOK, 128)
    out_ref[:, TOK:] = outs[1].astype(bf16).reshape(NX * NY, TOK, 128)


def mid_kernel(
    place_ref, parts_ref, res_ref, gain_ref, routing_ref, *refs
):
    sources, (disp_ref, mid_ref, pick_ref, w_ref, sems) = refs[:8], refs[8:]
    copies = [
        pltpu.make_async_copy(src, w_ref.at[i // 2, pl.ds(96 * (i % 2), 96)], sems.at[i])
        for i, src in enumerate(sources)
    ]
    for copy in copies:
        copy.start()
    y = place_ref[3]
    total = jnp.zeros((TOK, D), f32)
    for n, shift in enumerate((0, 1, 3, 2)):
        ya = lax.rem(y + (NY - shift), NY)
        larges = [parts_ref[i, ya, 0:TOK, :].astype(f32) for i in range(NX)]
        smalls = [parts_ref[i, ya, TOK : 2 * TOK, :].astype(f32) for i in range(NX)]

        def mixed(values, at, scale):
            tops = [s[:, at : at + 1] for s in smalls]
            top = functools.reduce(jnp.maximum, tops)
            ws = [
                (s[:, at + 1 : at + 2] + s[:, at + 2 : at + 3]) * jnp.exp2((t - top) * scale)
                for s, t in zip(smalls, tops)
            ]
            inv = 1.0 / functools.reduce(jnp.add, ws)
            return functools.reduce(jnp.add, [v * (w * inv) for v, w in zip(values, ws)])

        large = mixed(larges, 0, SCALE_L).astype(bf16)
        small = mixed(smalls, 3, SCALE_S)[:, 64:128].astype(bf16)
        heads = jnp.concatenate([large, small], axis=1)
        copies[2 * n].wait()
        copies[2 * n + 1].wait()
        partial = jnp.dot(heads, w_ref[n], preferred_element_type=f32)
        total = total + partial.astype(bf16).astype(f32)
    attention = total.astype(bf16).astype(f32)
    middle = (res_ref[...].astype(f32) + attention).astype(bf16)
    mid_ref[...] = middle
    wide = middle.astype(f32)
    scale = lax.rsqrt(jnp.mean(wide * wide, axis=1, keepdims=True) + EPS)
    normed = (wide * scale * gain_ref[...]).astype(bf16)

    lane = lax.broadcasted_iota(jnp.int32, (TOK, SLOTS), 1)
    named_by = routing_ref[...].astype(f32)
    r = [column(named_by[k : k + 1, :]).astype(jnp.int32) for k in range(2)]
    hit = [lane == rk for rk in r]
    named = jnp.where(hit[0] | hit[1], 1.0, 0.0)
    tri = jnp.where(
        lax.broadcasted_iota(jnp.int32, (TOK, TOK), 1)
        < lax.broadcasted_iota(jnp.int32, (TOK, TOK), 0),
        1.0,
        0.0,
    )
    earlier = jnp.dot(tri.astype(bf16), named.astype(bf16), preferred_element_type=f32)
    send = jnp.zeros((TOK, SLOTS), f32)
    for k in range(2):
        slot = jnp.sum(jnp.where(hit[k], earlier, 0.0), axis=1, keepdims=True)
        pick = jnp.where(lane == r[k] * CAP + slot.astype(jnp.int32), 1.0, 0.0)
        pick_ref[k] = pick.astype(bf16)
        send = send + pick
    disp = lax.dot_general(
        send.astype(bf16), normed, (((0,), (0,)), ((), ())), preferred_element_type=f32
    ).astype(bf16)
    for e in range(EXPERTS):
        disp_ref[e] = disp[CAP * e : CAP * e + CAP]


def load_kernel(a, b, c, out_a, out_b, out_c, sems):
    copies = [
        pltpu.make_async_copy(src, dst, sems.at[i])
        for i, (src, dst) in enumerate(((a, out_a), (b, out_b), (c, out_c)))
    ]
    for copy in copies:
        copy.start()
    for copy in copies:
        copy.wait()


def ffn_kernel(*refs):
    count = (len(refs) - 3) // 2
    xs, (wg, wu, wd), outs = refs[:count], refs[count : count + 3], refs[count + 3 :]
    rows = jnp.concatenate([x[...] for x in xs], axis=0) if count > 1 else xs[0][...]
    gate = jnp.dot(rows, wg[...], preferred_element_type=f32)
    up = jnp.dot(rows, wu[...], preferred_element_type=f32)
    m = jnp.minimum(gate, LIMIT)
    linear = jnp.clip(up, -LIMIT, LIMIT) + 1.0
    hidden = (m * jax.nn.sigmoid(ALPHA * m) * linear).astype(bf16)
    out = jnp.dot(hidden, wd[...], preferred_element_type=f32).astype(bf16)
    at = 0
    for x, o in zip(xs, outs):
        o[...] = out[at : at + x.shape[0]]
        at += x.shape[0]


def end_kernel(mid_ref, pick_ref, ret_ref, weight_ref, out_ref):
    total = mid_ref[...].astype(f32)
    ret = ret_ref[...]
    weight = weight_ref[...]
    mixed = column(weight[0:1, :]) * jnp.dot(pick_ref[0], ret, preferred_element_type=f32)
    mixed = mixed + column(weight[1:2, :]) * jnp.dot(
        pick_ref[1], ret, preferred_element_type=f32
    )
    out_ref[...] = (total + mixed).astype(bf16)


def call(kernel, in_specs, shapes, scratch=(), flops=0, mib=16):
    many = len(shapes) > 1
    outs = [jax.ShapeDtypeStruct(s, d) for s, d in shapes]
    return pl.pallas_call(
        kernel,
        in_specs=in_specs,
        out_specs=vmem(len(outs)) if many else vmem(1)[0],
        out_shape=outs if many else outs[0],
        scratch_shapes=list(scratch),
        compiler_params=pltpu.CompilerParams(vmem_limit_bytes=mib * 2**20),
        cost_estimate=pl.CostEstimate(flops=flops, transcendentals=0, bytes_accessed=0)
        if flops
        else None,
    )


def shifted(a, axis, size, by):
    return lax.ppermute(a, axis, [(i, (i + by) % size) for i in range(size)])


def layer(
    residual, query_small, query_large, latent, rotary_key, latent_gain,
    small_keys, small_values, large_keys, large_values, small_output, large_output,
    ffn_gain, gate_weights, up_weights, down_weights, routing, route_weight,
):
    place = jnp.stack([lax.axis_index(a) for a in ("z", "x", "c", "y")]).astype(jnp.int32)
    base, row = rope_parts()
    kv, q, top, low = call(
        pre_kernel,
        [smem()] + vmem(13),
        [((NZ, 416, 128), bf16), ((256, 128), bf16), ((96, D), bf16), ((96, D), bf16)],
        flops=10**9,
        mib=63,
    )(
        place, latent, latent_gain[None, :], rotary_key.T, query_small.T, query_large.T,
        small_keys.T, small_values.T, large_keys, large_values, base, row,
        large_output, small_output,
    )

    kvs = lax.all_to_all(kv, "z", 0, 0, tiled=True)

    qx = [q]
    for by in (1, -1, 2):
        qx.append(shifted(q, "x", NX, by))
    qc = shifted(jnp.stack(qx), "c", NC, 1)

    top_p = shifted(top, "y", NY, 1)
    low_m = shifted(low, "y", NY, -1)
    low_p = shifted(low, "y", NY, 1)
    top_m = shifted(top, "y", NY, -1)
    top_o = shifted(top_p, "y", NY, 1)
    low_o = shifted(low_m, "y", NY, -1)

    def attend(other, *queries):
        return call(
            functools.partial(attn_kernel, other),
            [smem()] + vmem(1 + len(queries)),
            [((NX, NY, 2 * TOK, 128), bf16)],
            scratch=[
                pltpu.VMEM((256, 1024), bf16),
                pltpu.VMEM((128, 1024), bf16),
                pltpu.VMEM((1024, 256), bf16),
                pltpu.VMEM((128, 1024), bf16),
            ],
            flops=2 * 10**9,
            mib=20,
        )(place, kvs, *queries).reshape(NX * NY, 2 * TOK, 128)

    theirs = attend(True, qc)
    theirs = shifted(theirs, "c", NC, 1)
    ours = attend(False, *qx)
    parts = call(merge_kernel, vmem(2), [((NX * NY, 2 * TOK, 128), bf16)], flops=5 * 10**8)(
        ours, theirs
    )
    parts = lax.all_to_all(
        parts.reshape(NX * NY * 2 * TOK, 128), ("x", "y"), 0, 0, tiled=True
    ).reshape(NX, NY, 2 * TOK, 128)

    disp, middle, pick = call(
        mid_kernel,
        [smem()] + vmem(4) + [pl.BlockSpec(memory_space=pltpu.HBM) for _ in range(8)],
        [((EXPERTS, CAP, D), bf16), ((TOK, D), bf16), ((2, TOK, SLOTS), bf16)],
        scratch=[pltpu.VMEM((NY, 192, D), bf16), pltpu.SemaphoreType.DMA((8,))],
        flops=2 * 10**9,
        mib=63,
    )(
        place, parts, residual, ffn_gain[None, :], routing.T,
        top, low, top_p, low_p, top_m, low_m, top_o, low_o,
    )

    sp = ("z", "x", "c")
    mine = lax.all_to_all(disp, sp, 0, 0, tiled=True)
    mine = mine.reshape(SLOTS, D)

    half = SLOTS // 2
    x_a, x_b = mine[:half], mine[half:]
    weights = call(
        load_kernel,
        [pl.BlockSpec(memory_space=pltpu.HBM) for _ in range(3)],
        [((D, FF_LOCAL), bf16), ((D, FF_LOCAL), bf16), ((FF_LOCAL, D), bf16)],
        scratch=[pltpu.SemaphoreType.DMA((3,))],
        flops=10**9,
        mib=8,
    )(gate_weights[0], up_weights[0], down_weights[0])

    def ffn(*pieces):
        return call(
            ffn_kernel,
            vmem(len(pieces) + 3),
            [(p.shape, bf16) for p in pieces],
            flops=3 * 10**9,
            mib=28,
        )(*pieces, *weights)

    p_a = shifted(x_a, "y", NY, 1)
    m_b = shifted(x_b, "y", NY, -1)
    p_b = shifted(x_b, "y", NY, 1)
    m_a = shifted(x_a, "y", NY, -1)
    o_a = shifted(p_a, "y", NY, 1)
    o_b = shifted(m_b, "y", NY, -1)
    r0_a, r0_b, r1_a, r1_b, r3_a, r3_b = ffn(x_a, x_b, p_a, p_b, m_a, m_b)
    r2_a, r2_b = ffn(o_a, o_b)

    from_m_b = shifted(r3_b, "y", NY, 1)
    from_p_a = shifted(r1_a, "y", NY, -1)
    t_a = shifted(r2_a, "y", NY, 1)
    t_b = shifted(r2_b, "y", NY, -1)
    r3_a = (r3_a.astype(f32) + t_a.astype(f32)).astype(bf16)
    r1_b = (r1_b.astype(f32) + t_b.astype(f32)).astype(bf16)
    from_m_a = shifted(r3_a, "y", NY, 1)
    from_p_b = shifted(r1_b, "y", NY, -1)
    done = jnp.concatenate(
        [
            r0_a.astype(f32) + from_m_a.astype(f32) + from_p_a.astype(f32),
            r0_b.astype(f32) + from_m_b.astype(f32) + from_p_b.astype(f32),
        ],
        axis=0,
    ).astype(bf16)
    ret = lax.all_to_all(done.reshape(EXPERTS, CAP, D), sp, 0, 0, tiled=True)
    return call(end_kernel, vmem(4), [((TOK, D), bf16)])(
        middle, pick, ret.reshape(SLOTS, D), route_weight.T
    )


def solution(mesh):
    fine = Mesh(mesh.devices.reshape(NZ, NX, NC, NY), ("z", "x", "c", "y"))
    sp = ("z", "x", "c")
    every = ("z", "x", "c", "y")
    return jax.shard_map(
        layer,
        mesh=fine,
        in_specs=(
            P(every, None),
            P(sp, "y"),
            P(sp, "y"),
            P(sp, None),
            P(sp, None),
            P(),
            P(None, "y"),
            P(None, "y"),
            P(None, "y"),
            P(None, "y"),
            P("y", None),
            P("y", None),
            P(),
            P(sp, None, "y"),
            P(sp, None, "y"),
            P(sp, "y", None),
            P(every, None),
            P(every, None),
        ),
        out_specs=P(every, None),
        check_vma=False,
    )
```

```python
import functools

import jax
import jax.numpy as jnp
import numpy as np
from jax import lax
from jax.experimental import pallas as pl
from jax.experimental.pallas import tpu as pltpu
from jax.sharding import Mesh
from jax.sharding import PartitionSpec as P

NZ, NX, NC, NY = 8, 4, 2, 4
NXC = NX * NC
ROWS = 128
TOK = 32
D = 2048
NOPE_S = 64
NOPE_L = 128
ROPE = 32
EXPERTS = 64
CAP = 2
SLOTS = EXPERTS * CAP
FF_LOCAL = 512
EPS = 1e-6
LIMIT = 7.0
ALPHA = 1.702
ROPE_BASE = 10000.0
MASKED = -float(2**99)
LOG2E = 1.4426950408889634
SCALE_S = (NOPE_S + ROPE) ** -0.5 * LOG2E
SCALE_L = (NOPE_L + ROPE) ** -0.5 * LOG2E


f32 = jnp.float32
bf16 = jnp.bfloat16


def rope_parts():
    freq = ROPE_BASE ** (-np.arange(ROPE // 2, dtype=np.float64) * (2.0 / ROPE))

    def table(places):
        angles = places[:, None].astype(np.float64) * freq[None, :]
        c, s = np.cos(angles), np.sin(angles)
        return np.concatenate([c, c, s, s], axis=1).astype(np.float32)

    return table(np.arange(64) * ROWS), np.ascontiguousarray(table(np.arange(ROWS)).T)


def vmem(n):
    return [pl.BlockSpec(memory_space=pltpu.VMEM) for _ in range(n)]


def column(row):
    n = row.shape[1]
    same = lax.broadcasted_iota(jnp.int32, (n, n), 0) == lax.broadcasted_iota(
        jnp.int32, (n, n), 1
    )
    return jnp.sum(jnp.where(same, row, 0.0), axis=1, keepdims=True)


def pre_kernel(
    lat_ref, gain_ref, rk_ref, qs_ref, ql_ref, ks_w, vs_w, kl_w, vl_w,
    base_ref, row_ref, kv_ref, q_ref,
):
    block = (lax.axis_index("z") * NX + lax.axis_index("x")) * NC + lax.axis_index("c")
    base = column(base_ref[pl.ds(block, 1), :])
    cb, sb = base[:ROPE], base[ROPE:]
    cr, sr = row_ref[:ROPE], row_ref[ROPE:]
    cos = cr * cb - sr * sb
    sin = sr * cb + cr * sb
    at = lax.broadcasted_iota(jnp.int32, (ROPE, ROWS), 0)
    sin = jnp.where(at < ROPE // 2, -sin, sin)

    def turned(v):
        v = v.astype(f32)
        swapped = jnp.concatenate([v[ROPE // 2 :], v[: ROPE // 2]], axis=0)
        return v * cos + swapped * sin

    lat = lat_ref[...].astype(f32)
    scale = lax.rsqrt(jnp.mean(lat * lat, axis=1, keepdims=True) + EPS)
    normed = (lat * scale * gain_ref[...]).astype(bf16)
    across = (((1,), (1,)), ((), ()))

    kv_ref[0, 0:128, :] = jnp.dot(normed, kl_w[...], preferred_element_type=f32).T.astype(bf16)
    kv_ref[0, 128:256, :] = jnp.dot(normed, vl_w[...], preferred_element_type=f32).astype(bf16)
    kv_ref[0, 256:320, :] = lax.dot_general(
        ks_w[...], normed, across, preferred_element_type=f32
    ).astype(bf16)
    kv_ref[0, 320:352, :] = turned(rk_ref[...]).astype(bf16)
    kv_ref[0, 352:416, :] = lax.dot_general(
        vs_w[...], normed, across, preferred_element_type=f32
    ).astype(bf16)
    for j in range(1, NZ):
        kv_ref[j] = kv_ref[0]
    q_ref[0:128, :] = ql_ref[0:NOPE_L, :].astype(f32).T.astype(bf16)
    mixed = jnp.concatenate(
        [qs_ref[0:NOPE_S, :].astype(f32), turned(ql_ref[NOPE_L:, :]), turned(qs_ref[NOPE_S:, :])],
        axis=0,
    )
    q_ref[128:256, :] = mixed.T.astype(bf16)


def attn_kernel(other, kv_ref, *refs):
    queries, (out_ref, kl, ks, vl, vs) = refs[:-5], refs[-5:]
    z, x, c = (lax.axis_index(a) for a in ("z", "x", "c"))
    kl[128:192, :] = jnp.zeros((64, 1024), bf16)
    kl[224:256, :] = jnp.zeros((32, 1024), bf16)
    ks[64:96, :] = jnp.zeros((32, 1024), bf16)
    vl[:, 128:256] = jnp.ones((1024, 128), bf16)
    vs[0:64, :] = jnp.ones((64, 1024), bf16)
    for j in range(NZ):
        lo, hi = j * ROWS, (j + 1) * ROWS
        rot = kv_ref[j, 320:352, :]
        kl[0:128, lo:hi] = kv_ref[j, 0:128, :]
        kl[192:224, lo:hi] = rot
        ks[0:64, lo:hi] = kv_ref[j, 256:320, :]
        ks[96:128, lo:hi] = rot
        vl[lo:hi, 0:128] = kv_ref[j, 128:256, :]
        vs[64:128, lo:hi] = kv_ref[j, 352:416, :]
    key = lax.broadcasted_iota(jnp.int32, (1, NZ * ROWS), 1)
    kpos = (key // ROWS) * (NXC * ROWS) + (x * NC + c) * ROWS + lax.rem(key, ROWS)
    row = lax.broadcasted_iota(jnp.int32, (2 * ROWS, 1), 0)
    lanes = lax.broadcasted_iota(jnp.int32, (2 * ROWS, 128), 1)
    core = 1 - c if other else c
    for d in (0, 2):
        block = [queries[0][d + i] if other else queries[d + i][...] for i in range(2)]
        xq = [lax.rem(x + (NX - s), NX) for s in ((0, 1) if d == 0 else (3, 2))]
        q = jnp.concatenate(
            [jnp.concatenate([b[0:128, :], b[128:256, :]], axis=1) for b in block], axis=0
        )
        qpos = z * (NXC * ROWS) + jnp.where(
            row < ROWS,
            (xq[0] * NC + core) * ROWS + row,
            (xq[1] * NC + core) * ROWS + row - ROWS,
        )
        allowed = kpos <= qpos

        def attend(query, keys, values, contract, scale, at):
            s = jnp.dot(query, keys[...], preferred_element_type=f32)
            s = jnp.where(allowed, s, MASKED)
            top = jnp.max(s, axis=1, keepdims=True).astype(bf16).astype(f32)
            w = jnp.exp2((s - top) * scale).astype(bf16)
            o = lax.dot_general(
                w, values[...], (((1,), (contract,)), ((), ())), preferred_element_type=f32
            )
            total = o[:, at : at + 1]
            return o[:, :128] / total, top, total

        o_l, m_l, t_l = attend(q, kl, vl, 0, SCALE_L, 128)
        o_s, m_s, t_s = attend(q[:, 128:256], ks, vs, 1, SCALE_S, 0)
        h_l = t_l.astype(bf16).astype(f32)
        h_s = t_s.astype(bf16).astype(f32)
        for i, v in enumerate((m_l, h_l, t_l - h_l, m_s, h_s, t_s - h_s)):
            o_s = jnp.where(lanes == i, v, o_s)
        o_l = o_l.astype(bf16)
        o_s = o_s.astype(bf16)
        for half in range(2):
            for y in range(NY):
                lo = half * ROWS + y * TOK
                out_ref[xq[half], y, 0:TOK, :] = o_l[lo : lo + TOK]
                out_ref[xq[half], y, TOK : 2 * TOK, :] = o_s[lo : lo + TOK]


def merge_kernel(a_ref, b_ref, out_ref):
    rows = NX * NY * TOK
    ref = [r[...].astype(f32) for r in (a_ref, b_ref)]
    large = [r[:, :TOK].reshape(rows, 128) for r in ref]
    small = [r[:, TOK:].reshape(rows, 128) for r in ref]
    lanes = lax.broadcasted_iota(jnp.int32, (rows, 128), 1)
    outs = []
    stats = []
    for at, scale, values in ((0, SCALE_L, large), (3, SCALE_S, small)):
        tops = [s[:, at : at + 1] for s in small]
        top = jnp.maximum(tops[0], tops[1])
        ws = [
            (s[:, at + 1 : at + 2] + s[:, at + 2 : at + 3]) * jnp.exp2((t - top) * scale)
            for s, t in zip(small, tops)
        ]
        total = ws[0] + ws[1]
        outs.append(values[0] * (ws[0] / total) + values[1] * (ws[1] / total))
        high = total.astype(bf16).astype(f32)
        stats += [top, high, total - high]
    for i, v in enumerate(stats):
        outs[1] = jnp.where(lanes == i, v, outs[1])
    out_ref[:, :TOK] = outs[0].astype(bf16).reshape(NX * NY, TOK, 128)
    out_ref[:, TOK:] = outs[1].astype(bf16).reshape(NX * NY, TOK, 128)


def gather_kernel(*refs):
    sources, (out_ref, sems) = refs[:8], refs[8:]
    copies = [
        pltpu.make_async_copy(
            src, out_ref.at[i // 2, pl.ds(128 * (i % 2), 128 - 64 * (i % 2))], sems.at[i]
        )
        for i, src in enumerate(sources)
    ]
    for copy in copies:
        copy.start()
    for copy in copies:
        copy.wait()


def mid_kernel(
    parts_ref, res_ref, gain_ref, routing_ref, w_ref, disp_ref, mid_ref, pick_ref
):
    y = lax.axis_index("y")
    total = jnp.zeros((TOK, D), f32)
    for n, shift in enumerate((0, 1, 3, 2)):
        ya = lax.rem(y + (NY - shift), NY)
        larges = [parts_ref[i, ya, 0:TOK, :].astype(f32) for i in range(NX)]
        smalls = [parts_ref[i, ya, TOK : 2 * TOK, :].astype(f32) for i in range(NX)]

        def mixed(values, at, scale):
            tops = [s[:, at : at + 1] for s in smalls]
            top = functools.reduce(jnp.maximum, tops)
            ws = [
                (s[:, at + 1 : at + 2] + s[:, at + 2 : at + 3]) * jnp.exp2((t - top) * scale)
                for s, t in zip(smalls, tops)
            ]
            inv = 1.0 / functools.reduce(jnp.add, ws)
            return functools.reduce(jnp.add, [v * (w * inv) for v, w in zip(values, ws)])

        large = mixed(larges, 0, SCALE_L).astype(bf16)
        small = mixed(smalls, 3, SCALE_S)[:, 64:128].astype(bf16)
        heads = jnp.concatenate([large, small], axis=1)
        partial = jnp.dot(heads, w_ref[n], preferred_element_type=f32)
        total = total + partial.astype(bf16).astype(f32)
    attention = total.astype(bf16).astype(f32)
    middle = (res_ref[...].astype(f32) + attention).astype(bf16)
    mid_ref[...] = middle
    wide = middle.astype(f32)
    scale = lax.rsqrt(jnp.mean(wide * wide, axis=1, keepdims=True) + EPS)
    normed = (wide * scale * gain_ref[...]).astype(bf16)

    lane = lax.broadcasted_iota(jnp.int32, (TOK, SLOTS), 1)
    named_by = routing_ref[...].astype(f32)
    r = [column(named_by[k : k + 1, :]).astype(jnp.int32) for k in range(2)]
    hit = [lane == rk for rk in r]
    named = jnp.where(hit[0] | hit[1], 1.0, 0.0)
    tri = jnp.where(
        lax.broadcasted_iota(jnp.int32, (TOK, TOK), 1)
        < lax.broadcasted_iota(jnp.int32, (TOK, TOK), 0),
        1.0,
        0.0,
    )
    earlier = jnp.dot(tri.astype(bf16), named.astype(bf16), preferred_element_type=f32)
    send = jnp.zeros((TOK, SLOTS), f32)
    for k in range(2):
        slot = jnp.sum(jnp.where(hit[k], earlier, 0.0), axis=1, keepdims=True)
        pick = jnp.where(lane == r[k] * CAP + slot.astype(jnp.int32), 1.0, 0.0)
        pick_ref[k] = pick.astype(bf16)
        send = send + pick
    disp = lax.dot_general(
        send.astype(bf16), normed, (((0,), (0,)), ((), ())), preferred_element_type=f32
    ).astype(bf16)
    for e in range(EXPERTS):
        disp_ref[e] = disp[CAP * e : CAP * e + CAP]


def load_kernel(a, b, c, out_a, out_b, out_c, sems):
    copies = [
        pltpu.make_async_copy(src, dst, sems.at[i])
        for i, (src, dst) in enumerate(((a, out_a), (b, out_b), (c, out_c)))
    ]
    for copy in copies:
        copy.start()
    for copy in copies:
        copy.wait()


def ffn_kernel(*refs):
    count = (len(refs) - 3) // 2
    xs, (wg, wu, wd), outs = refs[:count], refs[count : count + 3], refs[count + 3 :]
    rows = jnp.concatenate([x[...] for x in xs], axis=0) if count > 1 else xs[0][...]
    gate = jnp.dot(rows, wg[...], preferred_element_type=f32)
    up = jnp.dot(rows, wu[...], preferred_element_type=f32)
    m = jnp.minimum(gate, LIMIT)
    linear = jnp.clip(up, -LIMIT, LIMIT) + 1.0
    hidden = (m * jax.nn.sigmoid(ALPHA * m) * linear).astype(bf16)
    out = jnp.dot(hidden, wd[...], preferred_element_type=f32).astype(bf16)
    at = 0
    for x, o in zip(xs, outs):
        o[...] = out[at : at + x.shape[0]]
        at += x.shape[0]


def end_kernel(mid_ref, pick_ref, ret_ref, weight_ref, out_ref):
    total = mid_ref[...].astype(f32)
    ret = ret_ref[...]
    weight = weight_ref[...]
    mixed = column(weight[0:1, :]) * jnp.dot(pick_ref[0], ret, preferred_element_type=f32)
    mixed = mixed + column(weight[1:2, :]) * jnp.dot(
        pick_ref[1], ret, preferred_element_type=f32
    )
    out_ref[...] = (total + mixed).astype(bf16)


def call(kernel, in_specs, shapes, scratch=(), flops=0, mib=16):
    many = len(shapes) > 1
    outs = [jax.ShapeDtypeStruct(s, d) for s, d in shapes]
    return pl.pallas_call(
        kernel,
        in_specs=in_specs,
        out_specs=vmem(len(outs)) if many else vmem(1)[0],
        out_shape=outs if many else outs[0],
        scratch_shapes=list(scratch),
        compiler_params=pltpu.CompilerParams(vmem_limit_bytes=mib * 2**20),
        cost_estimate=pl.CostEstimate(flops=flops, transcendentals=0, bytes_accessed=0)
        if flops
        else None,
    )


def shifted(a, axis, size, by):
    return lax.ppermute(a, axis, [(i, (i + by) % size) for i in range(size)])


def layer(
    residual, query_small, query_large, latent, rotary_key, latent_gain,
    small_keys, small_values, large_keys, large_values, small_output, large_output,
    ffn_gain, gate_weights, up_weights, down_weights, routing, route_weight,
):
    base, row = rope_parts()
    kv, q = call(
        pre_kernel,
        vmem(11),
        [((NZ, 416, 128), bf16), ((256, 128), bf16)],
        flops=10**9,
        mib=63,
    )(
        latent, latent_gain[None, :], rotary_key.T, query_small.T, query_large.T,
        small_keys.T, small_values.T, large_keys, large_values, base, row,
    )

    kvs = lax.all_to_all(kv, "z", 0, 0, tiled=True)

    qx = [q]
    for by in (1, -1, 2):
        qx.append(shifted(q, "x", NX, by))
    qc = shifted(jnp.stack(qx), "c", NC, 1)

    top, low = large_output, small_output
    top_p = shifted(top, "y", NY, 1)
    low_m = shifted(low, "y", NY, -1)
    low_p = shifted(low, "y", NY, 1)
    top_m = shifted(top, "y", NY, -1)
    top_o = shifted(top_p, "y", NY, 1)
    low_o = shifted(low_m, "y", NY, -1)

    def attend(other, *queries):
        return call(
            functools.partial(attn_kernel, other),
            vmem(1 + len(queries)),
            [((NX, NY, 2 * TOK, 128), bf16)],
            scratch=[
                pltpu.VMEM((256, 1024), bf16),
                pltpu.VMEM((128, 1024), bf16),
                pltpu.VMEM((1024, 256), bf16),
                pltpu.VMEM((128, 1024), bf16),
            ],
            flops=2 * 10**9,
            mib=20,
        )(kvs, *queries).reshape(NX * NY, 2 * TOK, 128)

    theirs = attend(True, qc)
    theirs = shifted(theirs, "c", NC, 1)
    ours = attend(False, *qx)
    parts = call(merge_kernel, vmem(2), [((NX * NY, 2 * TOK, 128), bf16)], flops=5 * 10**8)(
        ours, theirs
    )
    parts = lax.all_to_all(
        parts.reshape(NX * NY * 2 * TOK, 128), ("x", "y"), 0, 0, tiled=True
    ).reshape(NX, NY, 2 * TOK, 128)
    projection = call(
        gather_kernel,
        [pl.BlockSpec(memory_space=pltpu.HBM) for _ in range(8)],
        [((NY, 192, D), bf16)],
        scratch=[pltpu.SemaphoreType.DMA((8,))],
        flops=10**9,
        mib=8,
    )(top, low, top_p, low_p, top_m, low_m, top_o, low_o)

    disp, middle, pick = call(
        mid_kernel,
        vmem(5),
        [((EXPERTS, CAP, D), bf16), ((TOK, D), bf16), ((2, TOK, SLOTS), bf16)],
        flops=2 * 10**9,
    )(parts, residual, ffn_gain[None, :], routing.T, projection)

    sp = ("z", "x", "c")
    mine = lax.all_to_all(disp, sp, 0, 0, tiled=True)
    mine = mine.reshape(SLOTS, D)

    half = SLOTS // 2
    x_a, x_b = mine[:half], mine[half:]
    weights = call(
        load_kernel,
        [pl.BlockSpec(memory_space=pltpu.HBM) for _ in range(3)],
        [((D, FF_LOCAL), bf16), ((D, FF_LOCAL), bf16), ((FF_LOCAL, D), bf16)],
        scratch=[pltpu.SemaphoreType.DMA((3,))],
        flops=10**9,
        mib=8,
    )(gate_weights[0], up_weights[0], down_weights[0])

    def ffn(*pieces):
        return call(
            ffn_kernel,
            vmem(len(pieces) + 3),
            [(p.shape, bf16) for p in pieces],
            flops=3 * 10**9,
            mib=28,
        )(*pieces, *weights)

    p_a = shifted(x_a, "y", NY, 1)
    m_b = shifted(x_b, "y", NY, -1)
    p_b = shifted(x_b, "y", NY, 1)
    m_a = shifted(x_a, "y", NY, -1)
    o_a = shifted(p_a, "y", NY, 1)
    o_b = shifted(m_b, "y", NY, -1)
    r0_a, r0_b, r1_a, r1_b, r3_a, r3_b = ffn(x_a, x_b, p_a, p_b, m_a, m_b)
    r2_a, r2_b = ffn(o_a, o_b)

    from_m_b = shifted(r3_b, "y", NY, 1)
    from_p_a = shifted(r1_a, "y", NY, -1)
    t_a = shifted(r2_a, "y", NY, 1)
    t_b = shifted(r2_b, "y", NY, -1)
    r3_a = (r3_a.astype(f32) + t_a.astype(f32)).astype(bf16)
    r1_b = (r1_b.astype(f32) + t_b.astype(f32)).astype(bf16)
    from_m_a = shifted(r3_a, "y", NY, 1)
    from_p_b = shifted(r1_b, "y", NY, -1)
    done = jnp.concatenate(
        [
            r0_a.astype(f32) + from_m_a.astype(f32) + from_p_a.astype(f32),
            r0_b.astype(f32) + from_m_b.astype(f32) + from_p_b.astype(f32),
        ],
        axis=0,
    ).astype(bf16)
    ret = lax.all_to_all(done.reshape(EXPERTS, CAP, D), sp, 0, 0, tiled=True)
    return call(end_kernel, vmem(4), [((TOK, D), bf16)])(
        middle, pick, ret.reshape(SLOTS, D), route_weight.T
    )


def solution(mesh):
    fine = Mesh(mesh.devices.reshape(NZ, NX, NC, NY), ("z", "x", "c", "y"))
    sp = ("z", "x", "c")
    every = ("z", "x", "c", "y")
    return jax.shard_map(
        layer,
        mesh=fine,
        in_specs=(
            P(every, None),
            P(sp, "y"),
            P(sp, "y"),
            P(sp, None),
            P(sp, None),
            P(),
            P(None, "y"),
            P(None, "y"),
            P(None, "y"),
            P(None, "y"),
            P("y", None),
            P("y", None),
            P(),
            P(sp, None, "y"),
            P(sp, None, "y"),
            P(sp, "y", None),
            P(every, None),
            P(every, None),
        ),
        out_specs=P(every, None),
        check_vma=False,
    )
```

```python
import functools

import jax
import jax.numpy as jnp
import numpy as np
from jax import lax
from jax.experimental import pallas as pl
from jax.experimental.pallas import tpu as pltpu
from jax.sharding import Mesh
from jax.sharding import PartitionSpec as P

NZ, NX, NC, NY = 8, 4, 2, 4
NXC = NX * NC
ROWS = 128
TOK = 32
D = 2048
NOPE_S = 64
NOPE_L = 128
ROPE = 32
EXPERTS = 64
CAP = 2
SLOTS = EXPERTS * CAP
FF_LOCAL = 512
EPS = 1e-6
LIMIT = 7.0
ALPHA = 1.702
ROPE_BASE = 10000.0
MASKED = -float(2**99)
LOG2E = 1.4426950408889634
SCALE_S = (NOPE_S + ROPE) ** -0.5 * LOG2E
SCALE_L = (NOPE_L + ROPE) ** -0.5 * LOG2E


f32 = jnp.float32
bf16 = jnp.bfloat16


def rope_parts():
    freq = ROPE_BASE ** (-np.arange(ROPE // 2, dtype=np.float64) * (2.0 / ROPE))

    def table(places):
        angles = places[:, None].astype(np.float64) * freq[None, :]
        c, s = np.cos(angles), np.sin(angles)
        return np.concatenate([c, c, s, s], axis=1).astype(np.float32)

    return table(np.arange(64) * ROWS), np.ascontiguousarray(table(np.arange(ROWS)).T)


def vmem(n):
    return [pl.BlockSpec(memory_space=pltpu.VMEM) for _ in range(n)]


def column(row):
    n = row.shape[1]
    same = lax.broadcasted_iota(jnp.int32, (n, n), 0) == lax.broadcasted_iota(
        jnp.int32, (n, n), 1
    )
    return jnp.sum(jnp.where(same, row, 0.0), axis=1, keepdims=True)


def turner(base_ref, row_ref):
    block = (lax.axis_index("z") * NX + lax.axis_index("x")) * NC + lax.axis_index("c")
    base = column(base_ref[pl.ds(block, 1), :])
    cb, sb = base[:ROPE], base[ROPE:]
    cr, sr = row_ref[:ROPE], row_ref[ROPE:]
    cos = cr * cb - sr * sb
    sin = sr * cb + cr * sb
    at = lax.broadcasted_iota(jnp.int32, (ROPE, ROWS), 0)
    sin = jnp.where(at < ROPE // 2, -sin, sin)

    def turned(v):
        v = v.astype(f32)
        swapped = jnp.concatenate([v[ROPE // 2 :], v[: ROPE // 2]], axis=0)
        return v * cos + swapped * sin

    return turned


def key_kernel(
    lat_ref, gain_ref, rk_ref, ks_w, vs_w, kl_w, vl_w, base_ref, row_ref, kv_ref
):
    turned = turner(base_ref, row_ref)
    lat = lat_ref[...].astype(f32)
    scale = lax.rsqrt(jnp.mean(lat * lat, axis=1, keepdims=True) + EPS)
    normed = (lat * scale * gain_ref[...]).astype(bf16)
    across = (((1,), (1,)), ((), ()))

    kv_ref[0, 0:128, :] = jnp.dot(normed, kl_w[...], preferred_element_type=f32).T.astype(bf16)
    kv_ref[0, 128:256, :] = jnp.dot(normed, vl_w[...], preferred_element_type=f32).astype(bf16)
    kv_ref[0, 256:320, :] = lax.dot_general(
        ks_w[...], normed, across, preferred_element_type=f32
    ).astype(bf16)
    kv_ref[0, 320:352, :] = turned(rk_ref[...]).astype(bf16)
    kv_ref[0, 352:416, :] = lax.dot_general(
        vs_w[...], normed, across, preferred_element_type=f32
    ).astype(bf16)
    for j in range(1, NZ):
        kv_ref[j] = kv_ref[0]


def query_kernel(qs_ref, ql_ref, base_ref, row_ref, q_ref):
    turned = turner(base_ref, row_ref)
    q_ref[0:128, :] = ql_ref[0:NOPE_L, :].astype(f32).T.astype(bf16)
    mixed = jnp.concatenate(
        [qs_ref[0:NOPE_S, :].astype(f32), turned(ql_ref[NOPE_L:, :]), turned(qs_ref[NOPE_S:, :])],
        axis=0,
    )
    q_ref[128:256, :] = mixed.T.astype(bf16)


def attn_kernel(other, kv_ref, *refs):
    queries, (out_ref, kl, ks, vl, vs) = refs[:-5], refs[-5:]
    z, x, c = (lax.axis_index(a) for a in ("z", "x", "c"))
    kl[128:192, :] = jnp.zeros((64, 1024), bf16)
    kl[224:256, :] = jnp.zeros((32, 1024), bf16)
    ks[64:96, :] = jnp.zeros((32, 1024), bf16)
    vl[:, 128:256] = jnp.ones((1024, 128), bf16)
    vs[0:64, :] = jnp.ones((64, 1024), bf16)
    for j in range(NZ):
        lo, hi = j * ROWS, (j + 1) * ROWS
        rot = kv_ref[j, 320:352, :]
        kl[0:128, lo:hi] = kv_ref[j, 0:128, :]
        kl[192:224, lo:hi] = rot
        ks[0:64, lo:hi] = kv_ref[j, 256:320, :]
        ks[96:128, lo:hi] = rot
        vl[lo:hi, 0:128] = kv_ref[j, 128:256, :]
        vs[64:128, lo:hi] = kv_ref[j, 352:416, :]
    key = lax.broadcasted_iota(jnp.int32, (1, NZ * ROWS), 1)
    kpos = (key // ROWS) * (NXC * ROWS) + (x * NC + c) * ROWS + lax.rem(key, ROWS)
    row = lax.broadcasted_iota(jnp.int32, (2 * ROWS, 1), 0)
    lanes = lax.broadcasted_iota(jnp.int32, (2 * ROWS, 128), 1)
    core = 1 - c if other else c
    for d in (0, 2):
        block = [queries[0][d + i] if other else queries[d + i][...] for i in range(2)]
        xq = [lax.rem(x + (NX - s), NX) for s in ((0, 1) if d == 0 else (3, 2))]
        q = jnp.concatenate(
            [jnp.concatenate([b[0:128, :], b[128:256, :]], axis=1) for b in block], axis=0
        )
        qpos = z * (NXC * ROWS) + jnp.where(
            row < ROWS,
            (xq[0] * NC + core) * ROWS + row,
            (xq[1] * NC + core) * ROWS + row - ROWS,
        )
        allowed = kpos <= qpos

        def attend(query, keys, values, contract, scale, at):
            s = jnp.dot(query, keys[...], preferred_element_type=f32)
            s = jnp.where(allowed, s, MASKED)
            top = jnp.max(s, axis=1, keepdims=True).astype(bf16).astype(f32)
            w = jnp.exp2((s - top) * scale).astype(bf16)
            o = lax.dot_general(
                w, values[...], (((1,), (contract,)), ((), ())), preferred_element_type=f32
            )
            total = o[:, at : at + 1]
            return o[:, :128] / total, top, total

        o_l, m_l, t_l = attend(q, kl, vl, 0, SCALE_L, 128)
        o_s, m_s, t_s = attend(q[:, 128:256], ks, vs, 1, SCALE_S, 0)
        h_l = t_l.astype(bf16).astype(f32)
        h_s = t_s.astype(bf16).astype(f32)
        for i, v in enumerate((m_l, h_l, t_l - h_l, m_s, h_s, t_s - h_s)):
            o_s = jnp.where(lanes == i, v, o_s)
        o_l = o_l.astype(bf16)
        o_s = o_s.astype(bf16)
        for half in range(2):
            for y in range(NY):
                lo = half * ROWS + y * TOK
                out_ref[xq[half], y, 0:TOK, :] = o_l[lo : lo + TOK]
                out_ref[xq[half], y, TOK : 2 * TOK, :] = o_s[lo : lo + TOK]


def merged(large, small):
    lane = lax.broadcasted_iota(jnp.int32, small[0].shape, 1)
    scale = jnp.where(lane < 3, SCALE_L, SCALE_S)
    top = functools.reduce(jnp.maximum, small)
    ws = [
        (pltpu.roll(s, 127, 1) + pltpu.roll(s, 126, 1)) * jnp.exp2((s - top) * scale)
        for s in small
    ]
    total = functools.reduce(jnp.add, ws)
    ws = [w / total for w in ws]
    out_l = functools.reduce(jnp.add, [v * w[:, 0:1] for v, w in zip(large, ws)])
    out_s = functools.reduce(jnp.add, [v * w[:, 3:4] for v, w in zip(small, ws)])
    return out_l, out_s, top, total, lane


def merge_kernel(a_ref, b_ref, out_ref):
    rows = NX * NY * TOK
    ref = [r[...].astype(f32) for r in (a_ref, b_ref)]
    out_l, out_s, top, total, lane = merged(
        [r[:, :TOK].reshape(rows, 128) for r in ref],
        [r[:, TOK:].reshape(rows, 128) for r in ref],
    )
    high = total.astype(bf16).astype(f32)
    out_s = jnp.where((lane == 0) | (lane == 3), top, out_s)
    out_s = jnp.where((lane == 1) | (lane == 4), pltpu.roll(high, 1, 1), out_s)
    out_s = jnp.where((lane == 2) | (lane == 5), pltpu.roll(total - high, 2, 1), out_s)
    out_ref[:, :TOK] = out_l.astype(bf16).reshape(NX * NY, TOK, 128)
    out_ref[:, TOK:] = out_s.astype(bf16).reshape(NX * NY, TOK, 128)


def gather_kernel(*refs):
    sources, (out_ref, sems) = refs[:8], refs[8:]
    copies = [
        pltpu.make_async_copy(
            src, out_ref.at[i // 2, pl.ds(128 * (i % 2), 128 - 64 * (i % 2))], sems.at[i]
        )
        for i, src in enumerate(sources)
    ]
    for copy in copies:
        copy.start()
    for copy in copies:
        copy.wait()


def mid_kernel(
    parts_ref, res_ref, gain_ref, routing_ref, w_ref, disp_ref, mid_ref, pick_ref
):
    y = lax.axis_index("y")
    total = jnp.zeros((TOK, D), f32)
    for n, shift in enumerate((0, 1, 3, 2)):
        ya = lax.rem(y + (NY - shift), NY)
        larges = [parts_ref[i, ya, 0:TOK, :].astype(f32) for i in range(NX)]
        smalls = [parts_ref[i, ya, TOK : 2 * TOK, :].astype(f32) for i in range(NX)]

        out_l, out_s, _, _, _ = merged(larges, smalls)
        large = out_l.astype(bf16)
        small = out_s[:, 64:128].astype(bf16)
        heads = jnp.concatenate([large, small], axis=1)
        partial = jnp.dot(heads, w_ref[n], preferred_element_type=f32)
        total = total + partial.astype(bf16).astype(f32)
    attention = total.astype(bf16).astype(f32)
    middle = (res_ref[...].astype(f32) + attention).astype(bf16)
    mid_ref[...] = middle
    wide = middle.astype(f32)
    scale = lax.rsqrt(jnp.mean(wide * wide, axis=1, keepdims=True) + EPS)
    normed = (wide * scale * gain_ref[...]).astype(bf16)

    lane = lax.broadcasted_iota(jnp.int32, (TOK, SLOTS), 1)
    named_by = routing_ref[...].astype(f32)
    r = [column(named_by[k : k + 1, :]).astype(jnp.int32) for k in range(2)]
    hit = [lane == rk for rk in r]
    named = jnp.where(hit[0] | hit[1], 1.0, 0.0)
    tri = jnp.where(
        lax.broadcasted_iota(jnp.int32, (TOK, TOK), 1)
        < lax.broadcasted_iota(jnp.int32, (TOK, TOK), 0),
        1.0,
        0.0,
    )
    earlier = jnp.dot(tri.astype(bf16), named.astype(bf16), preferred_element_type=f32)
    send = jnp.zeros((TOK, SLOTS), f32)
    for k in range(2):
        slot = jnp.sum(jnp.where(hit[k], earlier, 0.0), axis=1, keepdims=True)
        pick = jnp.where(lane == r[k] * CAP + slot.astype(jnp.int32), 1.0, 0.0)
        pick_ref[k] = pick.astype(bf16)
        send = send + pick
    disp = lax.dot_general(
        send.astype(bf16), normed, (((0,), (0,)), ((), ())), preferred_element_type=f32
    ).astype(bf16)
    for e in range(EXPERTS):
        disp_ref[e] = disp[CAP * e : CAP * e + CAP]


def load_kernel(a, b, c, out_a, out_b, out_c, sems):
    copies = [
        pltpu.make_async_copy(src, dst, sems.at[i])
        for i, (src, dst) in enumerate(((a, out_a), (b, out_b), (c, out_c)))
    ]
    for copy in copies:
        copy.start()
    for copy in copies:
        copy.wait()


def ffn_kernel(*refs):
    count = (len(refs) - 3) // 2
    xs, (wg, wu, wd), outs = refs[:count], refs[count : count + 3], refs[count + 3 :]
    rows = jnp.concatenate([x[...] for x in xs], axis=0) if count > 1 else xs[0][...]
    gate = jnp.dot(rows, wg[...], preferred_element_type=f32)
    up = jnp.dot(rows, wu[...], preferred_element_type=f32)
    m = jnp.minimum(gate, LIMIT)
    linear = jnp.clip(up, -LIMIT, LIMIT) + 1.0
    hidden = (m * jax.nn.sigmoid(ALPHA * m) * linear).astype(bf16)
    out = jnp.dot(hidden, wd[...], preferred_element_type=f32).astype(bf16)
    at = 0
    for x, o in zip(xs, outs):
        o[...] = out[at : at + x.shape[0]]
        at += x.shape[0]


def end_kernel(mid_ref, pick_ref, ret_ref, weight_ref, out_ref):
    total = mid_ref[...].astype(f32)
    ret = ret_ref[...]
    weight = weight_ref[...]
    mixed = column(weight[0:1, :]) * jnp.dot(pick_ref[0], ret, preferred_element_type=f32)
    mixed = mixed + column(weight[1:2, :]) * jnp.dot(
        pick_ref[1], ret, preferred_element_type=f32
    )
    out_ref[...] = (total + mixed).astype(bf16)


def call(kernel, in_specs, shapes, scratch=(), flops=0, mib=16):
    many = len(shapes) > 1
    outs = [jax.ShapeDtypeStruct(s, d) for s, d in shapes]
    return pl.pallas_call(
        kernel,
        in_specs=in_specs,
        out_specs=vmem(len(outs)) if many else vmem(1)[0],
        out_shape=outs if many else outs[0],
        scratch_shapes=list(scratch),
        compiler_params=pltpu.CompilerParams(vmem_limit_bytes=mib * 2**20),
        cost_estimate=pl.CostEstimate(flops=flops, transcendentals=0, bytes_accessed=0)
        if flops
        else None,
    )


def shifted(a, axis, size, by):
    return lax.ppermute(a, axis, [(i, (i + by) % size) for i in range(size)])


def layer(
    residual, query_small, query_large, latent, rotary_key, latent_gain,
    small_keys, small_values, large_keys, large_values, small_output, large_output,
    ffn_gain, gate_weights, up_weights, down_weights, routing, route_weight,
):
    base, row = rope_parts()
    kv = call(key_kernel, vmem(9), [((NZ, 416, 128), bf16)], flops=10**9, mib=63)(
        latent, latent_gain[None, :], rotary_key.T, small_keys.T, small_values.T,
        large_keys, large_values, base, row,
    )

    kvs = lax.all_to_all(kv, "z", 0, 0, tiled=True)

    q = call(query_kernel, vmem(4), [((256, 128), bf16)], flops=10**8, mib=63)(
        query_small.T, query_large.T, base, row
    )

    qx = [q]
    for by in (1, -1, 2):
        qx.append(shifted(q, "x", NX, by))
    qc = shifted(jnp.stack(qx), "c", NC, 1)

    top, low = large_output, small_output
    top_p = shifted(top, "y", NY, 1)
    low_m = shifted(low, "y", NY, -1)
    low_p = shifted(low, "y", NY, 1)
    top_m = shifted(top, "y", NY, -1)
    top_o = shifted(top_p, "y", NY, 1)
    low_o = shifted(low_m, "y", NY, -1)

    def attend(other, *queries):
        return call(
            functools.partial(attn_kernel, other),
            vmem(1 + len(queries)),
            [((NX, NY, 2 * TOK, 128), bf16)],
            scratch=[
                pltpu.VMEM((256, 1024), bf16),
                pltpu.VMEM((128, 1024), bf16),
                pltpu.VMEM((1024, 256), bf16),
                pltpu.VMEM((128, 1024), bf16),
            ],
            flops=2 * 10**9,
            mib=20,
        )(kvs, *queries).reshape(NX * NY, 2 * TOK, 128)

    theirs = attend(True, qc)
    theirs = shifted(theirs, "c", NC, 1)
    ours = attend(False, *qx)
    parts = call(merge_kernel, vmem(2), [((NX * NY, 2 * TOK, 128), bf16)], flops=5 * 10**8)(
        ours, theirs
    )
    parts = lax.all_to_all(
        parts.reshape(NX * NY * 2 * TOK, 128), ("x", "y"), 0, 0, tiled=True
    ).reshape(NX, NY, 2 * TOK, 128)
    projection = call(
        gather_kernel,
        [pl.BlockSpec(memory_space=pltpu.HBM) for _ in range(8)],
        [((NY, 192, D), bf16)],
        scratch=[pltpu.SemaphoreType.DMA((8,))],
        flops=10**9,
        mib=8,
    )(top, low, top_p, low_p, top_m, low_m, top_o, low_o)

    disp, middle, pick = call(
        mid_kernel,
        vmem(5),
        [((EXPERTS, CAP, D), bf16), ((TOK, D), bf16), ((2, TOK, SLOTS), bf16)],
        flops=2 * 10**9,
    )(parts, residual, ffn_gain[None, :], routing.T, projection)

    sp = ("z", "x", "c")
    mine = lax.all_to_all(disp, sp, 0, 0, tiled=True)
    mine = mine.reshape(SLOTS, D)

    half = SLOTS // 2
    x_a, x_b = mine[:half], mine[half:]
    weights = call(
        load_kernel,
        [pl.BlockSpec(memory_space=pltpu.HBM) for _ in range(3)],
        [((D, FF_LOCAL), bf16), ((D, FF_LOCAL), bf16), ((FF_LOCAL, D), bf16)],
        scratch=[pltpu.SemaphoreType.DMA((3,))],
        flops=10**9,
        mib=8,
    )(gate_weights[0], up_weights[0], down_weights[0])

    def ffn(*pieces):
        return call(
            ffn_kernel,
            vmem(len(pieces) + 3),
            [(p.shape, bf16) for p in pieces],
            flops=3 * 10**9,
            mib=28,
        )(*pieces, *weights)

    p_a = shifted(x_a, "y", NY, 1)
    m_b = shifted(x_b, "y", NY, -1)
    p_b = shifted(x_b, "y", NY, 1)
    m_a = shifted(x_a, "y", NY, -1)
    o_a = shifted(p_a, "y", NY, 1)
    o_b = shifted(m_b, "y", NY, -1)
    r0_a, r0_b, r1_a, r1_b, r3_a, r3_b = ffn(x_a, x_b, p_a, p_b, m_a, m_b)
    r2_a, r2_b = ffn(o_a, o_b)

    from_m_b = shifted(r3_b, "y", NY, 1)
    from_p_a = shifted(r1_a, "y", NY, -1)
    t_a = shifted(r2_a, "y", NY, 1)
    t_b = shifted(r2_b, "y", NY, -1)
    r3_a = (r3_a.astype(f32) + t_a.astype(f32)).astype(bf16)
    r1_b = (r1_b.astype(f32) + t_b.astype(f32)).astype(bf16)
    from_m_a = shifted(r3_a, "y", NY, 1)
    from_p_b = shifted(r1_b, "y", NY, -1)
    done = jnp.concatenate(
        [
            r0_a.astype(f32) + from_m_a.astype(f32) + from_p_a.astype(f32),
            r0_b.astype(f32) + from_m_b.astype(f32) + from_p_b.astype(f32),
        ],
        axis=0,
    ).astype(bf16)
    ret = lax.all_to_all(done.reshape(EXPERTS, CAP, D), sp, 0, 0, tiled=True)
    return call(end_kernel, vmem(4), [((TOK, D), bf16)])(
        middle, pick, ret.reshape(SLOTS, D), route_weight.T
    )


def solution(mesh):
    fine = Mesh(mesh.devices.reshape(NZ, NX, NC, NY), ("z", "x", "c", "y"))
    sp = ("z", "x", "c")
    every = ("z", "x", "c", "y")
    return jax.shard_map(
        layer,
        mesh=fine,
        in_specs=(
            P(every, None),
            P(sp, "y"),
            P(sp, "y"),
            P(sp, None),
            P(sp, None),
            P(),
            P(None, "y"),
            P(None, "y"),
            P(None, "y"),
            P(None, "y"),
            P("y", None),
            P("y", None),
            P(),
            P(sp, None, "y"),
            P(sp, None, "y"),
            P(sp, "y", None),
            P(every, None),
            P(every, None),
        ),
        out_specs=P(every, None),
        check_vma=False,
    )
```
